32 devices in a mesh: gr: 2 (over x), fs: 4 (over z), tp: 4 (over y, core).
Axes of the slice: x: 2, y: 2, z: 4, core: 2. Of those that a mesh axis runs over, the one named last changes fastest.
Arguments:
- prompt_tokens: bfloat16 [4096, 2048], P(('gr', 'fs', 'tp')), may hold values from -60 to 60
- norm_gain: float32 [2048], P(('gr', 'fs')), may hold values from 0.1 to 1.9
- up_master: float32 [2048, 8192], P(('gr', 'fs'), 'tp'), may hold values from -0.125 to 0.125
- down_master: float32 [2048, 8192], P(('gr', 'fs'), 'tp'), may hold values from -0.0625 to 0.0625
Outputs:
- up_served: bfloat16 [2048, 8192], P(None, 'tp')
- down_served: bfloat16 [2048, 8192], P(None, 'tp')
- mlp_output: bfloat16 [4096, 2048], P(('gr', 'fs', 'tp'))
The draws below stay inside these ranges and needn't reach their ends.
All inputs are finite; a program needn't handle non-finite values.
Results may differ from the reference program's by a relative error of at most 0.014.
Values may be sent and summed in bfloat16 or wider, within the bound.
A program may use at most 128 MiB of HBM per device.

```python
import math
import jax
import jax.numpy as jnp
from jax import lax

D = 2048
FF = 8192
TOKENS = 4096
N_TP = 4


def draw_prompt_tokens(key, part):
    entry_key, scale_key = jax.random.split(jax.random.fold_in(key, 17))
    entries = jnp.clip(jax.random.normal(entry_key, (TOKENS, D), jnp.float32), -5.0, 5.0)
    scales = jnp.exp(jax.random.uniform(scale_key, (TOKENS,), jnp.float32, 0.0, jnp.log(10.0)))
    return (entries * scales[:, None]).astype(jnp.bfloat16)


def level_of(key, dims, pieces, least, high):
    def one(axis_at, parts):
        steps = jax.random.uniform(jax.random.fold_in(jax.random.fold_in(key, 6), axis_at), (parts,), jnp.float32, least / len(pieces), high / len(pieces))
        return jnp.repeat(jnp.exp(steps), dims[axis_at] // parts).reshape((-1,) + (1,) * (len(dims) - axis_at - 1))

    level = one(*pieces[0])
    for cut in pieces[1:]:
        level = level * one(*cut)
    return level


def bell_draw(key, dims, spread, reach, shards=(), held_as=jnp.bfloat16):
    result = jax.random.normal(key, dims, jnp.float32) * spread
    if len(shards) > 0:
        result = level_of(key, dims, shards, -0.22, 0.18) * result
    return jnp.clip(result, min=-reach, max=reach).astype(held_as)


def setup_inputs(seed: int = 0) -> dict:
    seeds = jax.random.split(jax.random.key(seed), 5)
    prompt_tokens = draw_prompt_tokens(jax.random.fold_in(seeds[4], 71), 0)
    norm_gain = jnp.clip(1.0 + 0.18 * jax.random.normal(seeds[1], (D,), jnp.float32), 0.1, 1.9)
    up_master = bell_draw(seeds[2], (D, FF), D ** -0.5, 0.125, ((0, 8), (1, 4)), jnp.float32)
    down_master = bell_draw(seeds[3], (D, FF), FF ** -0.5, 0.0625, ((0, 8), (1, 4)), jnp.float32)
    return {"prompt_tokens": prompt_tokens, "norm_gain": norm_gain, "up_master": up_master, "down_master": down_master}


def reference(prompt_tokens, norm_gain, up_master, down_master):
    up_served = (up_master * norm_gain[:, None]).astype(jnp.bfloat16)
    down_served = down_master.astype(jnp.bfloat16)
    floats = prompt_tokens.astype(jnp.float32)
    mean_square = lax.optimization_barrier(lax.optimization_barrier(jnp.mean(floats * floats, axis=1, keepdims=True)))
    normed = (floats * lax.rsqrt(mean_square + 1e-06)).astype(jnp.bfloat16)
    block = math.gcd(TOKENS, 1024)
    width = FF // N_TP
    down_blocks = down_served.reshape(D, N_TP, width).astype(jnp.float32)

    def one_block(rows):
        pre = jnp.dot(rows, up_served, preferred_element_type=jnp.float32)
        hidden = jnp.square(jnp.maximum(pre, 0.0)).astype(jnp.bfloat16)
        split = hidden.reshape(block, N_TP, width).astype(jnp.float32)
        partial_value = jnp.einsum('rkf,dkf->krd', split, down_blocks).astype(jnp.bfloat16)
        partial_value = lax.optimization_barrier(partial_value)
        return lax.optimization_barrier(jnp.sum(partial_value.astype(jnp.float32), axis=0)).astype(jnp.bfloat16)
    outputs = lax.map(one_block, normed.reshape(TOKENS // block, block, D))
    return (up_served, down_served, outputs.reshape(TOKENS, D))
```

```python
import functools

import jax
import jax.numpy as jnp
from jax import lax
from jax.experimental import pallas as pl
from jax.experimental.pallas import tpu as pltpu
from jax.sharding import PartitionSpec as P

MESH = pl.DeviceIdType.MESH
CHUNK_BYTES = 256 * 1024
WRITES = 8


def pieces_of(rows, most):
    count = max(1, -(-rows // most))
    units = rows // 16
    cuts = [16 * (units * i // count) for i in range(count + 1)]
    return [(a, b - a) for a, b in zip(cuts, cuts[1:])]


def kernel(
    sizes, tok_hbm, gain_ref, up_hbm, down_hbm,
    up_ref, down_ref, out_ref,
    tok_ref, stage, normed, hidden, part, arrived,
    load_sem, tok_send, tok_recv,
    z_recv, right_send, left_send, x_recv, x_send, part_send, part_recv,
):
    n_gr, n_fs, n_tp = sizes
    g, z, t = lax.axis_index("gr"), lax.axis_index("fs"), lax.axis_index("tp")
    rows, width = stage.shape[1:]
    local = tok_ref.shape[0]
    depth = up_ref.shape[0]
    last = n_fs - 1
    has_right, has_left = z < last, z > 0
    masters = (up_ref, down_ref)

    def crossing(numerator):
        return max(16, rows * numerator // 256 * 16)

    most = max(16, CHUNK_BYTES // (2 * width) // 16 * 16)
    x_first = (crossing(3), crossing(3))
    tables = []
    for p in range(2):
        table = pieces_of(rows - x_first[p], most)
        tables.append(table + [(rows - x_first[p], x_first[p])] * 2)

    def at(p, col, zz, k):
        start, size = tables[p][k]
        base = pl.multiple_of((col * n_fs + zz) * rows, rows)
        return masters[p].at[pl.ds(pl.multiple_of(base + start, 16), size), :]

    def count(p):
        return len(tables[p]) - 2

    def z_copy(p, zz, k, right):
        col = 1 - g if k == count(p) + 1 else g
        ref = at(p, col, zz, k)
        send = right_send if right else left_send
        return pltpu.make_async_remote_copy(
            src_ref=ref, dst_ref=ref, send_sem=send.at[p, zz, k], recv_sem=z_recv.at[p, zz, k],
            device_id=(g, jnp.where(has_right, z + 1, z - 1) if right else jnp.where(has_left, z - 1, z + 1), t),
            device_id_type=MESH,
        )

    def x_copy(p, zz, k, col):
        ref = at(p, col, zz, k)
        return pltpu.make_async_remote_copy(
            src_ref=ref, dst_ref=ref, send_sem=x_send.at[p, zz, k], recv_sem=x_recv.at[p, zz, k],
            device_id=(1 - g, z, t), device_id_type=MESH,
        )

    def send_both(p, k):
        pl.when(has_right)(lambda: z_copy(p, z, k, True).start())
        pl.when(has_left)(lambda: z_copy(p, z, k, False).start())

    def own_z(p):
        for k in range(count(p) + 1):
            send_both(p, k)

    def own_x(p):
        x_copy(p, z, count(p), g).start()
        for k in range(count(p)):
            x_copy(p, z, k, g).start()

    def other_xz(p):
        x_copy(p, z, count(p), 1 - g).wait_recv()
        send_both(p, count(p) + 1)

    def slot(p, s, items=None):
        from_left, from_right = z - s >= 0, z + s <= last
        for k in range(count(p) + 2) if items is None else items:
            def left_in():
                z_copy(p, z - s, k, True).wait_recv()
                if s < last:
                    pl.when(has_right)(lambda: z_copy(p, z - s, k, True).start())
                if k < count(p):
                    x_copy(p, z - s, k, g).start()

            def right_in():
                z_copy(p, z + s, k, False).wait_recv()
                if s < last:
                    pl.when(has_left)(lambda: z_copy(p, z + s, k, False).start())
                if k < count(p):
                    x_copy(p, z + s, k, g).start()

            pl.when(from_left)(left_in)
            pl.when(from_right)(right_in)

    def token_copy(j):
        mine = normed.at[pl.ds(pl.multiple_of(t * local, local), local), :]
        return pltpu.make_async_remote_copy(
            src_ref=mine, dst_ref=mine, send_sem=tok_send.at[j - 1], recv_sem=tok_recv.at[j - 1],
            device_id=(g, z, lax.rem(t + j, n_tp)), device_id_type=MESH,
        )

    far = jnp.where(z + z >= last, 0, last)
    splits = (0, count(1) * 4 // 7, count(1) * 6 // 7, count(1))
    starts = [tables[1][k][0] for k in splits[:3]] + [rows]
    shares = [(a, b - a) for a, b in zip(starts, starts[1:])]
    whole_block = (0, rows)

    def part_copy(block, share, i, j):
        to = lax.rem(t + j, n_tp)
        start, size = share
        base = pl.multiple_of(block * rows, rows)
        row = pl.ds(pl.multiple_of(base + start, 16), size)
        return pltpu.make_async_remote_copy(
            src_ref=part.at[row, pl.ds(pl.multiple_of(to * local, local), local)],
            dst_ref=arrived.at[j - 1, row, :],
            send_sem=part_send.at[block, i, j - 1], recv_sem=part_recv.at[block, i, j - 1],
            device_id=(g, z, to), device_id_type=MESH,
        )

    def multiply(block, share, i):
        start, size = share
        base = pl.multiple_of(block * rows, rows)
        row = pl.ds(pl.multiple_of(base + start, 16), size)
        part[row, :] = lax.dot_general(
            down_ref[row, :], hidden[...], (((1,), (1,)), ((), ())),
            preferred_element_type=jnp.float32,
        ).astype(part.dtype)
        for j in range(1, n_tp):
            part_copy(block, share, i, j).start()

    def second(s):
        def one(i, carry):
            other, side = i // 2, lax.rem(i, 2)
            dist = s - other
            zz = z + (2 * side - 1) * dist
            ok = (dist >= 0) & (zz >= 0) & (zz <= last) & ((dist > 0) | (side == 0)) & (zz != far)

            @pl.when(ok)
            def _():
                @pl.when(other == 1)
                def _():
                    for k in range(count(1)):
                        x_copy(1, zz, k, 1 - g).wait_recv()

                multiply(jnp.where(other == 1, 1 - g, g) * n_fs + zz, whole_block, 0)

            return carry

        lax.fori_loop(0, 4, one, 0)

    def far_share(col, i):
        if shares[i][1] > 0:
            multiply(col * n_fs + far, shares[i], i)

    def far_x(i):
        for k in range(splits[i], splits[i + 1]):
            x_copy(1, far, k, 1 - g).wait_recv()

    def far_blocks():
        slot(1, last, range(splits[0], splits[1]))
        second(last)
        far_share(g, 0)
        slot(1, last, range(splits[1], splits[2]))
        far_x(0)
        far_share(1 - g, 0)
        far_share(g, 1)
        slot(1, last, range(splits[2], splits[3] + 1))
        far_share(g, 2)
        far_x(1)
        far_share(1 - g, 1)
        slot(1, last, range(splits[3] + 1, splits[3] + 2))
        far_x(2)
        far_share(1 - g, 2)

    def parts(b, act):
        @pl.when(lax.rem(b, n_fs) == far)
        def _():
            for i in range(3):
                if shares[i][1] > 0:
                    for j in range(1, n_tp):
                        act(part_copy(b, shares[i], i, j))

        @pl.when(lax.rem(b, n_fs) != far)
        def _():
            for j in range(1, n_tp):
                act(part_copy(b, whole_block, 0, j))

    loads = [
        pltpu.make_async_copy(up_hbm, stage.at[0], load_sem.at[0]),
        pltpu.make_async_copy(tok_hbm, tok_ref, load_sem.at[1]),
        pltpu.make_async_copy(down_hbm, stage.at[1], load_sem.at[2]),
    ]
    loads[0].start()
    loads[1].start()

    barrier = pltpu.get_barrier_semaphore()

    def greet(device):
        pl.semaphore_signal(barrier, inc=1, device_id=device, device_id_type=MESH)

    greet((1 - g, z, t))
    for j in range(1, n_tp):
        greet((g, z, lax.rem(t + j, n_tp)))
    pl.when(has_right)(lambda: greet((g, z + 1, t)))
    pl.when(has_left)(lambda: greet((g, z - 1, t)))

    def round_up(k):
        start, size = tables[0][k]
        row = pl.ds(pl.multiple_of((g * n_fs + z) * rows + start, 16), size)
        up_ref[row, :] = (stage[0, start : start + size] * gain[start : start + size]).astype(up_ref.dtype)

    def send_own(k):
        x_copy(0, z, k, g).start()
        if k < count(0):
            send_both(0, k)

    own = pl.ds(pl.multiple_of((g * n_fs + z) * rows, rows), rows)
    square = (rows, rows)
    on_diagonal = lax.broadcasted_iota(jnp.int32, square, 0) == lax.broadcasted_iota(jnp.int32, square, 1)
    gain = jnp.sum(jnp.where(on_diagonal, gain_ref[...], 0.0), axis=1, keepdims=True)
    loads[0].wait()
    order = [count(0)] + list(range(count(0)))
    round_up(order[0])
    round_up(order[1])
    pl.semaphore_wait(barrier, n_tp + has_right.astype(jnp.int32) + has_left.astype(jnp.int32))
    for i, k in enumerate(order):
        send_own(k)
        if i + 2 < len(order):
            round_up(order[i + 2])
    send_both(0, count(0))
    loads[2].start()

    loads[1].wait()
    floats = tok_ref[...].astype(jnp.float32)
    mean_square = jnp.mean(floats * floats, axis=1, keepdims=True)
    normed[pl.ds(pl.multiple_of(t * local, local), local), :] = (
        floats * lax.rsqrt(mean_square + 1e-06)
    ).astype(normed.dtype)
    for j in range(1, n_tp):
        token_copy(j).start()
    other_xz(0)
    loads[2].wait()
    down_ref[own, :] = stage[1].astype(down_ref.dtype)

    for s in range(1, last):
        slot(0, s)
    own_z(1)
    if last > 0:
        slot(0, last)
    own_x(1)

    for zz in range(n_fs):
        for k in range(count(0)):
            x_copy(0, zz, k, 1 - g).wait_recv()
    for j in range(1, n_tp):
        token_copy(j).wait_recv()

    tile = 256

    def first(i, carry):
        columns = pl.ds(pl.multiple_of(i * tile, tile), tile)
        pre = jnp.dot(normed[...], up_ref[:, columns], preferred_element_type=jnp.float32)
        hidden[:, columns] = jnp.square(jnp.maximum(pre, 0.0)).astype(hidden.dtype)
        return carry

    lax.fori_loop(0, width // tile, first, 0)

    other_xz(1)
    second(0)
    for s in range(1, last):
        slot(1, s)
        second(s)
    far_blocks()

    final = (1 - g) * n_fs + far
    last_tile = (final * rows + rows - 1) // 128

    def arrivals(b, carry):
        @pl.when(b != final)
        def _():
            parts(b, lambda copy: copy.wait_recv())

        return carry

    lax.fori_loop(0, n_gr * n_fs, arrivals, 0)
    for i in range(2):
        if shares[i][1] > 0:
            for j in range(1, n_tp):
                part_copy(final, shares[i], i, j).wait_recv()

    def total(i, carry):
        row = pl.ds(pl.multiple_of(i * 128, 128), 128)
        acc = part[row, pl.ds(pl.multiple_of(t * local, local), local)].astype(jnp.float32)
        for j in range(1, n_tp):
            acc = acc + arrived[j - 1, row, :].astype(jnp.float32)
        out_ref[:, row] = acc.T.astype(out_ref.dtype)
        return carry

    lax.fori_loop(0, last_tile, total, 0)
    lax.fori_loop(last_tile + 1, depth // 128, total, 0)

    def sent_parts(b, carry):
        parts(b, lambda copy: copy.wait_send())
        return carry

    lax.fori_loop(0, n_gr * n_fs, sent_parts, 0)
    for j in range(1, n_tp):
        token_copy(j).wait_send()

    def sent_blocks(zz, carry):
        for p in range(2):
            for k in range(count(p) + 2):
                pl.when(has_right & (zz <= z))(lambda: z_copy(p, zz, k, True).wait_send())
                pl.when(has_left & (zz >= z))(lambda: z_copy(p, zz, k, False).wait_send())
                if k < count(p):
                    x_copy(p, zz, k, g).wait_send()
                elif k == count(p):
                    pl.when(zz == z)(lambda: x_copy(p, zz, k, g).wait_send())
        return carry

    lax.fori_loop(0, n_fs, sent_blocks, 0)

    for j in range(1, n_tp):
        part_copy(final, shares[2], 2, j).wait_recv()
    total(last_tile, 0)


def write_out(*refs):
    held, outs, sem = refs[:3], refs[3:6], refs[6]
    copies = []
    for i, (src, dst) in enumerate(zip(held, outs)):
        rows = src.shape[0] // WRITES
        for k in range(WRITES):
            part = pl.ds(k * rows, rows)
            copies.append(pltpu.make_async_copy(src.at[part, :], dst.at[part, :], sem.at[i, k]))
    for copy in copies:
        copy.start()
    for copy in copies:
        copy.wait()


def solution(mesh):
    n_gr, n_fs, n_tp = (mesh.shape[a] for a in ("gr", "fs", "tp"))

    def on_device(prompt_tokens, norm_gain, up_master, down_master):
        local, depth = prompt_tokens.shape
        rows, width = up_master.shape
        blocks = n_gr * n_fs
        most = 2 + -(-rows // max(16, CHUNK_BYTES // (2 * width) // 16 * 16))
        dma = pltpu.SemaphoreType.DMA
        bf16 = jnp.bfloat16
        anywhere = pl.BlockSpec(memory_space=pl.ANY)
        vmem = pl.BlockSpec(memory_space=pltpu.VMEM)
        held = pl.pallas_call(
            functools.partial(kernel, (n_gr, n_fs, n_tp)),
            out_shape=(
                pltpu.VMEM((depth, width), bf16),
                pltpu.VMEM((depth, width), bf16),
                pltpu.VMEM((local, depth), bf16),
            ),
            in_specs=[anywhere, vmem, anywhere, anywhere],
            out_specs=(vmem, vmem, vmem),
            scratch_shapes=[
                pltpu.VMEM((local, depth), bf16),
                pltpu.VMEM((2, rows, width), jnp.float32),
                pltpu.VMEM((local * n_tp, depth), bf16),
                pltpu.VMEM((local * n_tp, width), bf16),
                pltpu.VMEM((depth, local * n_tp), bf16),
                pltpu.VMEM((n_tp - 1, depth, local), bf16),
                dma((3,)), dma((n_tp - 1,)), dma((n_tp - 1,)),
                dma((2, n_fs, most)), dma((2, n_fs, most)), dma((2, n_fs, most)),
                dma((2, n_fs, most)), dma((2, n_fs, most)),
                dma((blocks, 3, n_tp - 1)), dma((blocks, 3, n_tp - 1)),
            ],
            compiler_params=pltpu.CompilerParams(
                collective_id=0, has_side_effects=True, vmem_limit_bytes=44 * 2**20
            ),
        )(prompt_tokens, norm_gain[None, :], up_master, down_master)
        return pl.pallas_call(
            write_out,
            out_shape=(
                jax.ShapeDtypeStruct((depth, width), bf16),
                jax.ShapeDtypeStruct((depth, width), bf16),
                jax.ShapeDtypeStruct((local, depth), bf16),
            ),
            in_specs=[vmem, vmem, vmem],
            out_specs=(anywhere, anywhere, anywhere),
            scratch_shapes=[dma((3, WRITES))],
            compiler_params=pltpu.CompilerParams(vmem_limit_bytes=2**20),
        )(*held)

    placed = (
        P(("gr", "fs", "tp"), None),
        P(("gr", "fs")),
        P(("gr", "fs"), "tp"),
        P(("gr", "fs"), "tp"),
    )
    return jax.shard_map(
        on_device,
        mesh=mesh,
        in_specs=placed,
        out_specs=(P(None, "tp"), P(None, "tp"), P(("gr", "fs", "tp"), None)),
        check_vma=False,
    )
```

```python
import functools

import jax
import jax.numpy as jnp
from jax import lax
from jax.experimental import pallas as pl
from jax.experimental.pallas import tpu as pltpu
from jax.sharding import PartitionSpec as P

MESH = pl.DeviceIdType.MESH
CHUNK_BYTES = 256 * 1024
WRITES = 8
CROSSED = (3, 2)


def pieces_of(start, stop, most):
    rows = stop - start
    count = -(-rows // most)
    units = rows // 16
    cuts = [start + 16 * (units * i // count) for i in range(count)] + [stop]
    return [(a, b - a) for a, b in zip(cuts, cuts[1:])]


def split_rows(rows, width):
    most = max(16, CHUNK_BYTES // (2 * width) // 16 * 16)
    tail = max(0, rows - 128)
    tables = []
    for p in range(2):
        edge = rows - max(16, rows * CROSSED[p] // 256 * 16)
        cut = min(tail, edge) if p else edge
        near, rest, cross = pieces_of(0, cut, most), pieces_of(cut, edge, most), [(edge, rows - edge)]
        tables.append((near, rest, near + rest + cross + cross + rest))
    return tail, tables


def kernel(
    sizes, gain_hbm, tok_hbm, up_hbm, down_hbm,
    up_ref, down_ref, out_ref,
    tok_ref, gain_ref, stage, normed, hidden, part, arrived,
    far_hidden, far_part, far_arrived, far_out,
    load_sem, up_sem, tok_send, tok_recv,
    z_recv, right_send, left_send, x_recv, x_send, part_send, part_recv,
    hid_send, hid_recv, far_send, far_recv, give_send, give_recv,
):
    n_gr, n_fs, n_tp = sizes
    g, z, t = lax.axis_index("gr"), lax.axis_index("fs"), lax.axis_index("tp")
    rows, width = stage.shape[1:]
    local = tok_ref.shape[0]
    depth = up_ref.shape[0]
    last = n_fs - 1
    has_right, has_left = z < last, z > 0
    at_end = (z == 0) | (z == last)
    masters = (up_ref, down_ref)

    tail, tables = split_rows(rows, width)
    helped = n_fs >= 4 and rows % 128 == 0
    near = [range(len(a)) for a, _, _ in tables]
    rest = [range(len(a), len(a) + len(b)) for a, b, _ in tables]
    cross = [r.stop for r in rest]
    extra = [range(c + 2, c + 2 + len(r)) for c, r in zip(cross, rest)]

    def is_end(zz):
        return (zz == 0) | (zz == last)

    def rest_by_x(zz):
        return jnp.logical_not(is_end(zz)) | (zz == z) | (zz + z == last)

    def at(p, col, zz, k):
        start, size = tables[p][2][k]
        base = pl.multiple_of((col * n_fs + zz) * rows, rows)
        return masters[p].at[pl.ds(pl.multiple_of(base + start, 16), size), :]

    def z_copy(p, zz, k, right):
        ref = at(p, 1 - g if k > cross[p] else g, zz, k)
        send = right_send if right else left_send
        return pltpu.make_async_remote_copy(
            src_ref=ref, dst_ref=ref, send_sem=send.at[p, zz, k], recv_sem=z_recv.at[p, zz, k],
            device_id=(g, jnp.where(has_right, z + 1, z - 1) if right else jnp.where(has_left, z - 1, z + 1), t),
            device_id_type=MESH,
        )

    def x_copy(p, zz, k, col):
        ref = at(p, col, zz, k)
        return pltpu.make_async_remote_copy(
            src_ref=ref, dst_ref=ref, send_sem=x_send.at[p, zz, k], recv_sem=x_recv.at[p, zz, k],
            device_id=(1 - g, z, t), device_id_type=MESH,
        )

    def goes(p, zz, k, right):
        if k < cross[p] + 2:
            return has_right if right else has_left
        return (zz == 0) & (z + 1 < last) if right else (zz == last) & (z > 1)

    def send_both(p, k):
        pl.when(goes(p, z, k, True))(lambda: z_copy(p, z, k, True).start())
        pl.when(goes(p, z, k, False))(lambda: z_copy(p, z, k, False).start())

    def own_z(p):
        for k in range(cross[p] + 1):
            send_both(p, k)

    def own_x(p):
        for k in (cross[p], *rest[p], *near[p]):
            x_copy(p, z, k, g).start()

    def other_xz(p):
        x_copy(p, z, cross[p], 1 - g).wait_recv()
        send_both(p, cross[p] + 1)

    def other_rest(p):
        @pl.when(at_end)
        def _():
            for k, wide in zip(rest[p], extra[p]):
                x_copy(p, z, k, 1 - g).wait_recv()
                send_both(p, wide)

    def slot(p, s, items):
        for k in items:
            wide = k in extra[p]

            def come(right):
                zz = z - s if right else z + s
                z_copy(p, zz, k, right).wait_recv()
                if s < last:
                    pl.when(goes(p, zz, k, right))(lambda: z_copy(p, zz, k, right).start())
                if k in near[p]:
                    x_copy(p, zz, k, g).start()
                elif k in rest[p]:
                    pl.when(rest_by_x(zz))(lambda: x_copy(p, zz, k, g).start())

            from_left, from_right = z - s >= 0, z + s <= last
            if wide:
                from_left, from_right = (z - s == 0) & has_right, (z + s == last) & has_left
            if not wide or s < last:
                pl.when(from_left)(lambda: come(True))
                pl.when(from_right)(lambda: come(False))

    def whole_slot(p, s):
        slot(p, s, range(len(tables[p][2])))

    def token_copy(j):
        mine = normed.at[pl.ds(pl.multiple_of(t * local, local), local), :]
        return pltpu.make_async_remote_copy(
            src_ref=mine, dst_ref=mine, send_sem=tok_send.at[j - 1], recv_sem=tok_recv.at[j - 1],
            device_id=(g, z, lax.rem(t + j, n_tp)), device_id_type=MESH,
        )

    far = jnp.where(z + z >= last, 0, last)
    shares = [(0, tail), (tail, rows - tail)]
    whole_block = (0, rows)

    def part_copy(block, share, i, j):
        to = lax.rem(t + j, n_tp)
        start, size = share
        base = pl.multiple_of(block * rows, rows)
        row = pl.ds(pl.multiple_of(base + start, 16), size)
        return pltpu.make_async_remote_copy(
            src_ref=part.at[row, pl.ds(pl.multiple_of(to * local, local), local)],
            dst_ref=arrived.at[j - 1, row, :],
            send_sem=part_send.at[block, i, j - 1], recv_sem=part_recv.at[block, i, j - 1],
            device_id=(g, z, to), device_id_type=MESH,
        )

    def product(block, share, values):
        start, size = share
        base = pl.multiple_of(block * rows, rows)
        row = pl.ds(pl.multiple_of(base + start, 16), size)
        return row, lax.dot_general(
            down_ref[row, :], values[...], (((1,), (1,)), ((), ())),
            preferred_element_type=jnp.float32,
        ).astype(part.dtype)

    def multiply(block, share, i):
        row, value = product(block, share, hidden)
        part[row, :] = value
        for j in range(1, n_tp):
            part_copy(block, share, i, j).start()

    def second(s):
        def one(i, carry):
            other, side = i // 2, lax.rem(i, 2)
            dist = s - other
            zz = z + (2 * side - 1) * dist
            ok = (dist >= 0) & (zz >= 0) & (zz <= last) & ((dist > 0) | (side == 0)) & (zz != far)

            @pl.when(ok)
            def _():
                @pl.when(other == 1)
                def _():
                    for k in near[1]:
                        x_copy(1, zz, k, 1 - g).wait_recv()

                    @pl.when(jnp.logical_not(is_end(zz)))
                    def _():
                        for k in rest[1]:
                            x_copy(1, zz, k, 1 - g).wait_recv()

                multiply(jnp.where(other == 1, 1 - g, g) * n_fs + zz, whole_block, 0)

            return carry

        lax.fori_loop(0, 4, one, 0)

    def far_share(col, i):
        if shares[i][1] > 0:
            multiply(col * n_fs + far, shares[i], i)

    def far_tails():
        far_share(g, 1)
        far_share(1 - g, 1)

    tail_here = jnp.logical_not(at_end) if helped else z >= 0
    helping = (z == 1) | (z == last - 1)
    helper = jnp.where(z == 0, 1, last - 1)
    ward = jnp.where(z == 1, 0, last)

    def hidden_copy(i):
        row = pl.ds(i * local, local)
        return pltpu.make_async_remote_copy(
            src_ref=hidden.at[row, :], dst_ref=far_hidden.at[row, :],
            send_sem=hid_send.at[i], recv_sem=hid_recv.at[i],
            device_id=(g, helper, t), device_id_type=MESH,
        )

    def far_copy(col, j):
        to = lax.rem(t + j, n_tp)
        row = pl.ds(col * 128, 128)
        return pltpu.make_async_remote_copy(
            src_ref=far_part.at[row, pl.ds(pl.multiple_of(to * local, local), local)],
            dst_ref=far_arrived.at[j - 1, row, :],
            send_sem=far_send.at[col, j - 1], recv_sem=far_recv.at[col, j - 1],
            device_id=(g, z, to), device_id_type=MESH,
        )

    def give_copy(col):
        column = pl.ds(pl.multiple_of((col * n_fs + far) * rows + tail, 128), 128)
        return pltpu.make_async_remote_copy(
            src_ref=far_out.at[col], dst_ref=out_ref.at[:, column],
            send_sem=give_send.at[col], recv_sem=give_recv.at[col],
            device_id=(g, ward, t), device_id_type=MESH,
        )

    def help_multiply():
        for i in range(n_tp):
            hidden_copy(i).wait_recv()
        for col in range(2):
            _, value = product(col * n_fs + far, shares[1], far_hidden)
            far_part[pl.ds(col * 128, 128), :] = value
            for j in range(1, n_tp):
                far_copy(col, j).start()

    def help_total():
        for col in range(2):
            for j in range(1, n_tp):
                far_copy(col, j).wait_recv()
            row = pl.ds(col * 128, 128)
            acc = far_part[row, pl.ds(pl.multiple_of(t * local, local), local)].astype(jnp.float32)
            for j in range(1, n_tp):
                acc = acc + far_arrived[j - 1, row, :].astype(jnp.float32)
            far_out[col] = acc.T.astype(far_out.dtype)
            give_copy(col).start()

    def parts(b, act, final_too=True):
        @pl.when(lax.rem(b, n_fs) == far)
        def _():
            if shares[0][1] > 0:
                for j in range(1, n_tp):
                    if final_too:
                        act(part_copy(b, shares[0], 0, j))
                    else:
                        pl.when(b != final)(lambda: act(part_copy(b, shares[0], 0, j)))

            @pl.when(tail_here)
            def _():
                for j in range(1, n_tp):
                    act(part_copy(b, shares[1], 1, j))

        @pl.when(lax.rem(b, n_fs) != far)
        def _():
            for j in range(1, n_tp):
                act(part_copy(b, whole_block, 0, j))

    barrier = pltpu.get_barrier_semaphore()

    def greet(device):
        pl.semaphore_signal(barrier, inc=1, device_id=device, device_id_type=MESH)

    greet((1 - g, z, t))
    pl.when(has_right)(lambda: greet((g, z + 1, t)))
    pl.when(has_left)(lambda: greet((g, z - 1, t)))
    for j in range(1, n_tp):
        greet((g, z, lax.rem(t + j, n_tp)))

    order = [cross[0], *near[0]]

    def up_load(k):
        start, size = tables[0][2][k]
        row = pl.ds(start, size)
        return pltpu.make_async_copy(up_hbm.at[row, :], stage.at[0, row, :], up_sem.at[k])

    loads = [
        pltpu.make_async_copy(gain_hbm, gain_ref, load_sem.at[0]),
        pltpu.make_async_copy(tok_hbm, tok_ref, load_sem.at[1]),
        pltpu.make_async_copy(down_hbm, stage.at[1], load_sem.at[2]),
    ]
    loads[0].start()
    for k in order:
        up_load(k).start()
    loads[1].start()
    loads[2].start()

    def round_up(k):
        start, size = tables[0][2][k]
        row = pl.ds(pl.multiple_of((g * n_fs + z) * rows + start, 16), size)
        up_load(k).wait()
        up_ref[row, :] = (stage[0, start : start + size] * gain[start : start + size]).astype(up_ref.dtype)

    def send_own(k):
        x_copy(0, z, k, g).start()
        if k != cross[0]:
            send_both(0, k)

    own = pl.ds(pl.multiple_of((g * n_fs + z) * rows, rows), rows)
    square = (rows, rows)
    on_diagonal = lax.broadcasted_iota(jnp.int32, square, 0) == lax.broadcasted_iota(jnp.int32, square, 1)
    loads[0].wait()
    gain = jnp.sum(jnp.where(on_diagonal, gain_ref[...], 0.0), axis=1, keepdims=True)
    round_up(order[0])
    round_up(order[1])
    pl.semaphore_wait(barrier, n_tp + has_right.astype(jnp.int32) + has_left.astype(jnp.int32))
    for i, k in enumerate(order):
        send_own(k)
        if i + 2 < len(order):
            round_up(order[i + 2])
    send_both(0, cross[0])

    loads[1].wait()
    floats = tok_ref[...].astype(jnp.float32)
    mean_square = jnp.mean(floats * floats, axis=1, keepdims=True)
    normed[pl.ds(pl.multiple_of(t * local, local), local), :] = (
        floats * lax.rsqrt(mean_square + 1e-06)
    ).astype(normed.dtype)
    for j in range(1, n_tp):
        token_copy(j).start()
    other_xz(0)
    loads[2].wait()
    down_ref[own, :] = stage[1].astype(down_ref.dtype)

    for s in range(1, last):
        whole_slot(0, s)
    own_z(1)
    if last > 0:
        slot(0, last, near[0])
    own_x(1)
    if last > 0:
        slot(0, last, range(cross[0], cross[0] + 2))

    for zz in range(n_fs):
        for k in near[0]:
            x_copy(0, zz, k, 1 - g).wait_recv()
    for j in range(1, n_tp):
        token_copy(j).wait_recv()

    tile = 256

    def first(i, carry):
        columns = pl.ds(pl.multiple_of(i * tile, tile), tile)
        pre = jnp.dot(normed[...], up_ref[:, columns], preferred_element_type=jnp.float32)
        hidden[:, columns] = jnp.square(jnp.maximum(pre, 0.0)).astype(hidden.dtype)
        return carry

    lax.fori_loop(0, width // tile, first, 0)

    other_xz(1)
    other_rest(1)
    if helped:
        @pl.when(at_end)
        def _():
            for i in range(n_tp):
                hidden_copy(i).start()

    second(0)
    for s in range(1, last):
        whole_slot(1, s)
        second(s)
    slot(1, last, near[1])
    second(last)
    far_share(g, 0)
    slot(1, last, rest[1])
    if helped:
        pl.when(tail_here)(far_tails)
        pl.when(helping)(help_multiply)
    for k in near[1]:
        x_copy(1, far, k, 1 - g).wait_recv()
    far_share(1 - g, 0)
    if helped:
        pl.when(helping)(help_total)

    def last_in():
        slot(1, last, range(cross[1], cross[1] + 2))

        @pl.when(at_end)
        def _():
            for k in rest[1]:
                x_copy(1, far, k, 1 - g).wait_recv()

    if not helped:
        last_in()
        far_tails()

    final = (1 - g) * n_fs + far
    final_tile = final * (rows // 128)
    last_tile = final_tile + tail // 128

    def arrivals(b, carry):
        parts(b, lambda copy: copy.wait_recv(), False)
        return carry

    lax.fori_loop(0, n_gr * n_fs, arrivals, 0)

    def total(i, carry):
        row = pl.ds(pl.multiple_of(i * 128, 128), 128)
        acc = part[row, pl.ds(pl.multiple_of(t * local, local), local)].astype(jnp.float32)
        for j in range(1, n_tp):
            acc = acc + arrived[j - 1, row, :].astype(jnp.float32)
        out_ref[:, row] = acc.T.astype(out_ref.dtype)
        return carry

    def total_if(i, carry):
        is_tail = (lax.rem(i * 128, rows) == tail) & (lax.rem(i * 128 // rows, n_fs) == far)

        @pl.when(tail_here | jnp.logical_not(is_tail))
        def _():
            total(i, 0)

        return carry

    lax.fori_loop(0, final_tile, total_if, 0)
    lax.fori_loop(last_tile, depth // 128, total_if, 0)

    def sent_parts(b, carry):
        parts(b, lambda copy: copy.wait_send())
        return carry

    if shares[0][1] > 0:
        for j in range(1, n_tp):
            part_copy(final, shares[0], 0, j).wait_recv()
    lax.fori_loop(final_tile, last_tile, total, 0)
    lax.fori_loop(0, n_gr * n_fs, sent_parts, 0)
    for j in range(1, n_tp):
        token_copy(j).wait_send()
    if helped:
        @pl.when(at_end)
        def _():
            for i in range(n_tp):
                hidden_copy(i).wait_send()

        @pl.when(helping)
        def _():
            for col in range(2):
                for j in range(1, n_tp):
                    far_copy(col, j).wait_send()

    def sent_blocks(zz, carry):
        for p in range(2):
            for k in range(len(tables[p][2])):
                pl.when(goes(p, zz, k, True) & (zz <= z))(lambda: z_copy(p, zz, k, True).wait_send())
                pl.when(goes(p, zz, k, False) & (zz >= z))(lambda: z_copy(p, zz, k, False).wait_send())
                if k in near[p]:
                    x_copy(p, zz, k, g).wait_send()
                elif k in rest[p]:
                    pl.when(rest_by_x(zz))(lambda: x_copy(p, zz, k, g).wait_send())
                elif k == cross[p]:
                    pl.when(zz == z)(lambda: x_copy(p, zz, k, g).wait_send())
        return carry

    lax.fori_loop(0, n_fs, sent_blocks, 0)
    if helped:
        last_in()

        @pl.when(at_end)
        def _():
            for col in range(2):
                give_copy(col).wait_recv()

        @pl.when(helping)
        def _():
            for col in range(2):
                give_copy(col).wait_send()


def write_out(*refs):
    held, outs, sem = refs[:3], refs[3:6], refs[6]
    copies = []
    for i, (src, dst) in enumerate(zip(held, outs)):
        rows = src.shape[0] // WRITES
        for k in range(WRITES):
            part = pl.ds(k * rows, rows)
            copies.append(pltpu.make_async_copy(src.at[part, :], dst.at[part, :], sem.at[i, k]))
    for copy in copies:
        copy.start()
    for copy in copies:
        copy.wait()


def solution(mesh):
    n_gr, n_fs, n_tp = (mesh.shape[a] for a in ("gr", "fs", "tp"))

    def on_device(prompt_tokens, norm_gain, up_master, down_master):
        local, depth = prompt_tokens.shape
        rows, width = up_master.shape
        blocks = n_gr * n_fs
        most = max(len(table) for _, _, table in split_rows(rows, width)[1])
        dma = pltpu.SemaphoreType.DMA
        bf16 = jnp.bfloat16
        anywhere = pl.BlockSpec(memory_space=pl.ANY)
        vmem = pl.BlockSpec(memory_space=pltpu.VMEM)
        held = pl.pallas_call(
            functools.partial(kernel, (n_gr, n_fs, n_tp)),
            out_shape=(
                pltpu.VMEM((depth, width), bf16),
                pltpu.VMEM((depth, width), bf16),
                pltpu.VMEM((local, depth), bf16),
            ),
            in_specs=[anywhere] * 4,
            out_specs=(vmem, vmem, vmem),
            scratch_shapes=[
                pltpu.VMEM((local, depth), bf16),
                pltpu.VMEM((1, rows), jnp.float32),
                pltpu.VMEM((2, rows, width), jnp.float32),
                pltpu.VMEM((local * n_tp, depth), bf16),
                pltpu.VMEM((local * n_tp, width), bf16),
                pltpu.VMEM((depth, local * n_tp), bf16),
                pltpu.VMEM((n_tp - 1, depth, local), bf16),
                pltpu.VMEM((local * n_tp, width), bf16),
                pltpu.VMEM((256, local * n_tp), bf16),
                pltpu.VMEM((n_tp - 1, 256, local), bf16),
                pltpu.VMEM((2, local, 128), bf16),
                dma((3,)), dma((most,)), dma((n_tp - 1,)), dma((n_tp - 1,)),
                dma((2, n_fs, most)), dma((2, n_fs, most)), dma((2, n_fs, most)),
                dma((2, n_fs, most)), dma((2, n_fs, most)),
                dma((blocks, 2, n_tp - 1)), dma((blocks, 2, n_tp - 1)),
                dma((n_tp,)), dma((n_tp,)),
                dma((2, n_tp - 1)), dma((2, n_tp - 1)), dma((2,)), dma((2,)),
            ],
            compiler_params=pltpu.CompilerParams(
                collective_id=0, has_side_effects=True, vmem_limit_bytes=44 * 2**20
            ),
        )(norm_gain[None, :], prompt_tokens, up_master, down_master)
        return pl.pallas_call(
            write_out,
            out_shape=(
                jax.ShapeDtypeStruct((depth, width), bf16),
                jax.ShapeDtypeStruct((depth, width), bf16),
                jax.ShapeDtypeStruct((local, depth), bf16),
            ),
            in_specs=[vmem, vmem, vmem],
            out_specs=(anywhere, anywhere, anywhere),
            scratch_shapes=[dma((3, WRITES))],
            compiler_params=pltpu.CompilerParams(vmem_limit_bytes=2**20),
        )(*held)

    placed = (
        P(("gr", "fs", "tp"), None),
        P(("gr", "fs")),
        P(("gr", "fs"), "tp"),
        P(("gr", "fs"), "tp"),
    )
    return jax.shard_map(
        on_device,
        mesh=mesh,
        in_specs=placed,
        out_specs=(P(None, "tp"), P(None, "tp"), P(("gr", "fs", "tp"), None)),
        check_vma=False,
    )
```

```python
import functools

import jax
import jax.numpy as jnp
from jax import lax
from jax.experimental import pallas as pl
from jax.experimental.pallas import tpu as pltpu
from jax.sharding import PartitionSpec as P

MESH = pl.DeviceIdType.MESH
PIECES = (3, 2, 1)
WRITES = 4


def pieces_of(start, stop, count):
    units = (stop - start) // 8
    cuts = [start + 8 * (units * i // count) for i in range(count)] + [stop]
    return [(a, b - a) for a, b in zip(cuts, cuts[1:]) if b > a]


def split_rows(rows):
    tail = max(0, rows - 128)
    edge = rows - max(8, rows * 5 // 256 * 8)
    tables = []
    for cut, pieces in ((edge, PIECES[0]), (min(tail, edge), PIECES[1])):
        near, rest, cross = pieces_of(0, cut, pieces), pieces_of(cut, edge, PIECES[2]), [(edge, rows - edge)]
        tables.append((near, rest, near + rest + cross + cross + rest))
    return tail, tables


def kernel(
    sizes, gain_hbm, tok_hbm, up_hbm, down_hbm,
    up_ref, down_ref, out_ref,
    tok_ref, gain_ref, stage, normed, hidden, part, arrived,
    far_hidden, far_part, far_arrived, far_out,
    load_sem, up_sem, tok_sem,
    z_recv, right_send, left_send, x_recv, x_send, part_send, part_recv,
    hid_sem, far_sem, give_sem,
):
    n_gr, n_fs, n_tp = sizes
    g, z, t = lax.axis_index("gr"), lax.axis_index("fs"), lax.axis_index("tp")
    rows, width = stage.shape[1:]
    local = tok_ref.shape[0]
    depth = up_ref.shape[0]
    last = n_fs - 1
    has_right, has_left = z < last, z > 0
    at_end = (z == 0) | (z == last)
    masters = (up_ref, down_ref)

    tail, tables = split_rows(rows)
    helped = n_fs >= 4 and rows % 128 == 0
    near = [range(len(a)) for a, _, _ in tables]
    rest = [range(len(a), len(a) + len(b)) for a, b, _ in tables]
    cross = [r.stop for r in rest]
    extra = [range(c + 2, c + 2 + len(r)) for c, r in zip(cross, rest)]

    def inner(zz):
        return (zz != 0) & (zz != last)

    def rest_by_x(zz, here):
        return inner(zz) | (zz == here) | (zz + here == last)

    def goes(p, zz, k, right, here):
        if k < cross[p] + 2:
            return here < last if right else here > 0
        return (zz == 0) & (here + 1 < last) if right else (zz == last) & (here > 1)

    def settled(ref, sem):
        pltpu.make_async_copy(ref, ref, sem).wait()

    def settled_rows(count, sem):
        if count:
            settled(up_ref.at[pl.ds(0, count), :], sem)

    def size_of(p, items):
        return sum(tables[p][2][k][1] for k in items)

    def at(p, col, zz, k):
        start, size = tables[p][2][k]
        base = pl.multiple_of((col * n_fs + zz) * rows, rows)
        return masters[p].at[pl.ds(pl.multiple_of(base + start, 8), size), :]

    def z_copy(p, zz, k, right):
        ref = at(p, 1 - g if k > cross[p] else g, zz, k)
        send = right_send if right else left_send
        return pltpu.make_async_remote_copy(
            src_ref=ref, dst_ref=ref, send_sem=send.at[p], recv_sem=z_recv.at[p, zz if right else zz - 1, k],
            device_id=(g, jnp.where(has_right, z + 1, z - 1) if right else jnp.where(has_left, z - 1, z + 1), t),
            device_id_type=MESH,
        )

    def x_sem(p, zz, k):
        if k == cross[p]:
            return x_recv.at[p]
        if p == 0:
            return x_recv.at[2]
        return x_recv.at[3 + zz + (0 if k in near[1] else n_fs)]

    def x_copy(p, zz, k, col):
        ref = at(p, col, zz, k)
        return pltpu.make_async_remote_copy(
            src_ref=ref, dst_ref=ref, send_sem=x_send.at[p], recv_sem=x_sem(p, zz, k),
            device_id=(1 - g, z, t), device_id_type=MESH,
        )

    def send_both(p, k):
        pl.when(goes(p, z, k, True, z))(lambda: z_copy(p, z, k, True).start())
        pl.when(goes(p, z, k, False, z))(lambda: z_copy(p, z, k, False).start())

    def own_z(p):
        for k in range(cross[p] + 1):
            send_both(p, k)

    def own_x(p):
        for k in (cross[p], *rest[p], *near[p]):
            x_copy(p, z, k, g).start()

    def other_xz(p):
        x_copy(p, z, cross[p], 1 - g).wait_recv()
        send_both(p, cross[p] + 1)

    def near_in(zz):
        settled_rows(size_of(1, near[1]), x_recv.at[3 + zz])

    def rest_in(zz):
        settled_rows(size_of(1, rest[1]), x_recv.at[3 + n_fs + zz])

    def other_rest(p):
        @pl.when(at_end)
        def _():
            rest_in(z)
            for wide in extra[p]:
                send_both(p, wide)

    def slot(p, s, items):
        for k in items:
            wide = k in extra[p]

            def come(right):
                zz = z - s if right else z + s
                z_copy(p, zz, k, right).wait_recv()
                if s < last:
                    pl.when(goes(p, zz, k, right, z))(lambda: z_copy(p, zz, k, right).start())
                if k in near[p]:
                    x_copy(p, zz, k, g).start()
                elif k in rest[p]:
                    pl.when(rest_by_x(zz, z))(lambda: x_copy(p, zz, k, g).start())

            from_left, from_right = z - s >= 0, z + s <= last
            if wide:
                from_left, from_right = (z - s == 0) & has_right, (z + s == last) & has_left
            if not wide or s < last:
                pl.when(from_left)(lambda: come(True))
                pl.when(from_right)(lambda: come(False))

    def whole_slot(p, s):
        slot(p, s, range(len(tables[p][2])))

    def token_copy(j):
        mine = normed.at[pl.ds(pl.multiple_of(t * local, local), local), :]
        return pltpu.make_async_remote_copy(
            src_ref=mine, dst_ref=mine, send_sem=tok_sem.at[0], recv_sem=tok_sem.at[1],
            device_id=(g, z, lax.rem(t + j, n_tp)), device_id_type=MESH,
        )

    far = jnp.where(z + z >= last, 0, last)
    shares = [(0, tail), (tail, rows - tail)]
    whole_block = (0, rows)

    def part_copy(block, share, j, final):
        to = lax.rem(t + j, n_tp)
        start, size = share
        base = pl.multiple_of(block * rows, rows)
        row = pl.ds(pl.multiple_of(base + start, 16), size)
        return pltpu.make_async_remote_copy(
            src_ref=part.at[row, pl.ds(pl.multiple_of(to * local, local), local)],
            dst_ref=arrived.at[j - 1, row, :],
            send_sem=part_send.at[0], recv_sem=part_recv.at[1 if final else 0],
            device_id=(g, z, to), device_id_type=MESH,
        )

    def product(block, share, values):
        start, size = share
        base = pl.multiple_of(block * rows, rows)
        row = pl.ds(pl.multiple_of(base + start, 16), size)
        return row, lax.dot_general(
            down_ref[row, :], values[...], (((1,), (1,)), ((), ())),
            preferred_element_type=jnp.float32,
        ).astype(part.dtype)

    def multiply(block, share, final=False):
        row, value = product(block, share, hidden)
        part[row, :] = value
        for j in range(1, n_tp):
            part_copy(block, share, j, final).start()

    def second(s):
        def one(i, carry):
            other, side = i // 2, lax.rem(i, 2)
            dist = s - other
            zz = z + (2 * side - 1) * dist
            ok = (dist >= 0) & (zz >= 0) & (zz <= last) & ((dist > 0) | (side == 0)) & (zz != far)

            @pl.when(ok)
            def _():
                @pl.when(other == 1)
                def _():
                    near_in(zz)
                    pl.when(inner(zz))(lambda: rest_in(zz))

                multiply(jnp.where(other == 1, 1 - g, g) * n_fs + zz, whole_block)

            return carry

        lax.fori_loop(0, 4, one, 0)

    def far_share(col, i, final=False):
        if shares[i][1] > 0:
            multiply(col * n_fs + far, shares[i], final)

    def far_tails():
        far_share(g, 1)
        far_share(1 - g, 1)

    tail_here = jnp.logical_not(at_end) if helped else z >= 0
    helping = (z == 1) | (z == last - 1)
    helper = jnp.where(z == 0, 1, last - 1)
    ward = jnp.where(z == 1, 0, last)

    def hidden_copy():
        return pltpu.make_async_remote_copy(
            src_ref=hidden, dst_ref=far_hidden, send_sem=hid_sem.at[0], recv_sem=hid_sem.at[1],
            device_id=(g, helper, t), device_id_type=MESH,
        )

    def far_copy(col, j):
        to = lax.rem(t + j, n_tp)
        row = pl.ds(col * 128, 128)
        return pltpu.make_async_remote_copy(
            src_ref=far_part.at[row, pl.ds(pl.multiple_of(to * local, local), local)],
            dst_ref=far_arrived.at[j - 1, row, :],
            send_sem=far_sem.at[0], recv_sem=far_sem.at[1],
            device_id=(g, z, to), device_id_type=MESH,
        )

    def give_copy(col):
        column = pl.ds(pl.multiple_of((col * n_fs + far) * rows + tail, 128), 128)
        return pltpu.make_async_remote_copy(
            src_ref=far_out.at[col], dst_ref=out_ref.at[:, column],
            send_sem=give_sem.at[0], recv_sem=give_sem.at[1],
            device_id=(g, ward, t), device_id_type=MESH,
        )

    def help_multiply():
        hidden_copy().wait_recv()
        for col in range(2):
            _, value = product(col * n_fs + far, shares[1], far_hidden)
            far_part[pl.ds(col * 128, 128), :] = value
            for j in range(1, n_tp):
                far_copy(col, j).start()

    def help_total():
        settled(far_arrived, far_sem.at[1])
        for col in range(2):
            row = pl.ds(col * 128, 128)
            acc = far_part[row, pl.ds(pl.multiple_of(t * local, local), local)].astype(jnp.float32)
            for j in range(1, n_tp):
                acc = acc + far_arrived[j - 1, row, :].astype(jnp.float32)
            far_out[col] = acc.T.astype(far_out.dtype)
            give_copy(col).start()

    def parts_settled(final_rows, sem):
        every = depth - final_rows
        if not helped:
            settled(arrived.at[:, pl.ds(0, every), :], sem)
            return
        pl.when(at_end)(lambda: settled(arrived.at[:, pl.ds(0, every - 256), :], sem))
        pl.when(tail_here)(lambda: settled(arrived.at[:, pl.ds(0, every), :], sem))

    barrier = pltpu.get_barrier_semaphore()

    def greet(device):
        pl.semaphore_signal(barrier, inc=1, device_id=device, device_id_type=MESH)

    greet((1 - g, z, t))
    pl.when(has_right)(lambda: greet((g, z + 1, t)))
    pl.when(has_left)(lambda: greet((g, z - 1, t)))
    for j in range(1, n_tp):
        greet((g, z, lax.rem(t + j, n_tp)))

    order = [cross[0], *near[0]]

    def up_load(k):
        start, size = tables[0][2][k]
        row = pl.ds(start, size)
        return pltpu.make_async_copy(up_hbm.at[row, :], stage.at[0, row, :], up_sem.at[k])

    loads = [
        pltpu.make_async_copy(gain_hbm, gain_ref, load_sem.at[0]),
        pltpu.make_async_copy(tok_hbm, tok_ref, load_sem.at[1]),
        pltpu.make_async_copy(down_hbm, stage.at[1], load_sem.at[2]),
    ]
    loads[0].start()
    for k in order:
        up_load(k).start()
    loads[1].start()
    loads[2].start()

    def round_up(k):
        start, size = tables[0][2][k]
        row = pl.ds(pl.multiple_of((g * n_fs + z) * rows + start, 8), size)
        up_load(k).wait()
        up_ref[row, :] = (stage[0, start : start + size] * gain[start : start + size]).astype(up_ref.dtype)

    def send_own(k):
        x_copy(0, z, k, g).start()
        if k != cross[0]:
            send_both(0, k)

    own = pl.ds(pl.multiple_of((g * n_fs + z) * rows, rows), rows)
    square = (rows, rows)
    on_diagonal = lax.broadcasted_iota(jnp.int32, square, 0) == lax.broadcasted_iota(jnp.int32, square, 1)
    loads[0].wait()
    gain = jnp.sum(jnp.where(on_diagonal, gain_ref[...], 0.0), axis=1, keepdims=True)
    round_up(order[0])
    round_up(order[1])
    pl.semaphore_wait(barrier, n_tp + has_right.astype(jnp.int32) + has_left.astype(jnp.int32))
    for i, k in enumerate(order):
        send_own(k)
        if i + 2 < len(order):
            round_up(order[i + 2])
    send_both(0, cross[0])

    loads[1].wait()
    floats = tok_ref[...].astype(jnp.float32)
    mean_square = jnp.mean(floats * floats, axis=1, keepdims=True)
    normed[pl.ds(pl.multiple_of(t * local, local), local), :] = (
        floats * lax.rsqrt(mean_square + 1e-06)
    ).astype(normed.dtype)
    for j in range(1, n_tp):
        token_copy(j).start()
    other_xz(0)
    loads[2].wait()
    down_ref[own, :] = stage[1].astype(down_ref.dtype)

    for s in range(1, last):
        whole_slot(0, s)
    own_z(1)
    if last > 0:
        slot(0, last, near[0])
    own_x(1)
    if last > 0:
        slot(0, last, range(cross[0], cross[0] + 2))

    settled_rows(n_fs * size_of(0, near[0]), x_recv.at[2])
    others = normed.at[pl.ds(0, (n_tp - 1) * local), :]
    settled(others, tok_sem.at[1])

    tile = 256

    def first(i, carry):
        columns = pl.ds(pl.multiple_of(i * tile, tile), tile)
        pre = jnp.dot(normed[...], up_ref[:, columns], preferred_element_type=jnp.float32)
        hidden[:, columns] = jnp.square(jnp.maximum(pre, 0.0)).astype(hidden.dtype)
        return carry

    lax.fori_loop(0, width // tile, first, 0)

    other_xz(1)
    other_rest(1)
    if helped:
        @pl.when(at_end)
        def _():
            hidden_copy().start()

    second(0)
    for s in range(1, last):
        whole_slot(1, s)
        second(s)
    slot(1, last, near[1])
    second(last)
    far_share(g, 0)
    slot(1, last, rest[1])
    if helped:
        pl.when(tail_here)(far_tails)
        pl.when(helping)(help_multiply)
    near_in(far)
    far_share(1 - g, 0, True)
    if helped:
        pl.when(helping)(help_total)

    def last_in():
        slot(1, last, range(cross[1], cross[1] + 2))

        pl.when(at_end)(lambda: rest_in(far))

    if not helped:
        last_in()
        far_tails()

    final = (1 - g) * n_fs + far
    final_tile = final * (rows // 128)
    last_tile = final_tile + tail // 128

    parts_settled(tail, part_recv.at[0])

    def total(i, carry):
        row = pl.ds(pl.multiple_of(i * 128, 128), 128)
        acc = part[row, pl.ds(pl.multiple_of(t * local, local), local)].astype(jnp.float32)
        for j in range(1, n_tp):
            acc = acc + arrived[j - 1, row, :].astype(jnp.float32)
        out_ref[:, row] = acc.T.astype(out_ref.dtype)
        return carry

    def total_if(i, carry):
        is_tail = (lax.rem(i * 128, rows) == tail) & (lax.rem(i * 128 // rows, n_fs) == far)

        @pl.when(tail_here | jnp.logical_not(is_tail))
        def _():
            total(i, 0)

        return carry

    lax.fori_loop(0, final_tile, total_if, 0)
    lax.fori_loop(last_tile, depth // 128, total_if, 0)

    if tail > 0:
        settled(arrived.at[:, pl.ds(0, tail), :], part_recv.at[1])
    lax.fori_loop(final_tile, last_tile, total, 0)
    parts_settled(0, part_send.at[0])
    settled(others, tok_sem.at[0])
    if helped:
        pl.when(at_end)(lambda: hidden_copy().wait_send())
        pl.when(helping)(lambda: settled(far_arrived, far_sem.at[0]))

    def sent_blocks(here):
        for p in range(2):
            right = left = across = 0
            for zz in range(n_fs):
                for k, (_, size) in enumerate(tables[p][2]):
                    right += size * (zz <= here and goes(p, zz, k, True, here))
                    left += size * (zz >= here and goes(p, zz, k, False, here))
                    by_x = k in near[p] or (k in rest[p] and rest_by_x(zz, here)) or (k == cross[p] and zz == here)
                    across += size * by_x
            settled_rows(right, right_send.at[p])
            settled_rows(left, left_send.at[p])
            settled_rows(across, x_send.at[p])

    for here in range(n_fs):
        pl.when(z == here)(functools.partial(sent_blocks, here))
    if helped:
        last_in()

        pl.when(at_end)(lambda: settled(far_out, give_sem.at[1]))
        pl.when(helping)(lambda: settled(far_out, give_sem.at[0]))


def write_out(*refs):
    held, outs, sem = refs[:3], refs[3:6], refs[6]
    for i, (src, dst) in enumerate(zip(held, outs)):
        rows = src.shape[0] // WRITES
        for k in range(WRITES):
            part = pl.ds(k * rows, rows)
            pltpu.make_async_copy(src.at[part, :], dst.at[part, :], sem.at[i]).start()
    for i, (src, dst) in enumerate(zip(held, outs)):
        pltpu.make_async_copy(src, dst, sem.at[i]).wait()


def solution(mesh):
    n_gr, n_fs, n_tp = (mesh.shape[a] for a in ("gr", "fs", "tp"))

    def on_device(prompt_tokens, norm_gain, up_master, down_master):
        local, depth = prompt_tokens.shape
        rows, width = up_master.shape
        tables = split_rows(rows)[1]
        most = max(len(table) for _, _, table in tables)
        dma = pltpu.SemaphoreType.DMA
        bf16 = jnp.bfloat16
        anywhere = pl.BlockSpec(memory_space=pl.ANY)
        vmem = pl.BlockSpec(memory_space=pltpu.VMEM)
        held = pl.pallas_call(
            functools.partial(kernel, (n_gr, n_fs, n_tp)),
            out_shape=(
                pltpu.VMEM((depth, width), bf16),
                pltpu.VMEM((depth, width), bf16),
                pltpu.VMEM((local, depth), bf16),
            ),
            in_specs=[anywhere] * 4,
            out_specs=(vmem, vmem, vmem),
            scratch_shapes=[
                pltpu.VMEM((local, depth), bf16),
                pltpu.VMEM((1, rows), jnp.float32),
                pltpu.VMEM((2, rows, width), jnp.float32),
                pltpu.VMEM((local * n_tp, depth), bf16),
                pltpu.VMEM((local * n_tp, width), bf16),
                pltpu.VMEM((depth, local * n_tp), bf16),
                pltpu.VMEM((n_tp - 1, depth, local), bf16),
                pltpu.VMEM((local * n_tp, width), bf16),
                pltpu.VMEM((256, local * n_tp), bf16),
                pltpu.VMEM((n_tp - 1, 256, local), bf16),
                pltpu.VMEM((2, local, 128), bf16),
                dma((3,)), dma((most,)), dma((2,)),
                dma((2, max(1, n_fs - 1), most)), dma((2,)), dma((2,)), dma((3 + 2 * n_fs,)), dma((2,)),
                dma((1,)), dma((2,)), dma((2,)), dma((2,)), dma((2,)),
            ],
            compiler_params=pltpu.CompilerParams(
                collective_id=0, has_side_effects=True, vmem_limit_bytes=44 * 2**20
            ),
        )(norm_gain[None, :], prompt_tokens, up_master, down_master)
        return pl.pallas_call(
            write_out,
            out_shape=(
                jax.ShapeDtypeStruct((depth, width), bf16),
                jax.ShapeDtypeStruct((depth, width), bf16),
                jax.ShapeDtypeStruct((local, depth), bf16),
            ),
            in_specs=[vmem, vmem, vmem],
            out_specs=(anywhere, anywhere, anywhere),
            scratch_shapes=[dma((3,))],
            compiler_params=pltpu.CompilerParams(vmem_limit_bytes=2**20),
        )(*held)

    placed = (
        P(("gr", "fs", "tp"), None),
        P(("gr", "fs")),
        P(("gr", "fs"), "tp"),
        P(("gr", "fs"), "tp"),
    )
    return jax.shard_map(
        on_device,
        mesh=mesh,
        in_specs=placed,
        out_specs=(P(None, "tp"), P(None, "tp"), P(("gr", "fs", "tp"), None)),
        check_vma=False,
    )
```

```python
import functools

import jax
import jax.numpy as jnp
from jax import lax
from jax.experimental import pallas as pl
from jax.experimental.pallas import tpu as pltpu
from jax.sharding import PartitionSpec as P

MESH = pl.DeviceIdType.MESH
PIECES = (3, 2, 1)
WRITES = 4


def pieces_of(start, stop, count):
    units = (stop - start) // 8
    cuts = [start + 8 * (units * i // count) for i in range(count)] + [stop]
    return [(a, b - a) for a, b in zip(cuts, cuts[1:]) if b > a]


def split_rows(rows, width):
    def wide(pieces):
        return [(start, size, 0, width) for start, size in pieces]

    tail = max(0, rows - 128)
    edge = rows - max(8, rows * 5 // 256 * 8)
    near, cross = wide(pieces_of(0, edge, PIECES[0])), wide([(edge, rows - edge)])
    tables = [(near, [], near + cross + cross)]
    edge = rows - max(8, rows * 6 // 256 * 8)
    column = width * 7 // 8 // 128 * 128
    cut = min(tail, edge)
    near, rest = wide(pieces_of(0, cut, PIECES[1])), wide(pieces_of(cut, edge, PIECES[2]))
    rest.append((edge, rows - edge, column, width - column))
    cross = [(edge, rows - edge, 0, column)]
    tables.append((near, rest, near + rest + cross + cross + rest))
    return tail, tables


def kernel(
    sizes, gain_hbm, tok_hbm, up_hbm, down_hbm,
    up_ref, down_ref, out_ref,
    tok_ref, gain_ref, stage, normed, hidden, part, arrived,
    far_hidden, far_part, far_arrived, far_out,
    load_sem, up_sem, tok_sem,
    z_recv, right_send, left_send, x_recv, x_send, part_send, part_recv,
    hid_sem, far_sem, give_sem,
):
    n_gr, n_fs, n_tp = sizes
    g, z, t = lax.axis_index("gr"), lax.axis_index("fs"), lax.axis_index("tp")
    rows, width = stage.shape[1:]
    local = tok_ref.shape[0]
    depth = up_ref.shape[0]
    last = n_fs - 1
    has_right, has_left = z < last, z > 0
    at_end = (z == 0) | (z == last)
    masters = (up_ref, down_ref)

    tail, tables = split_rows(rows, width)
    helped = n_fs >= 4 and rows % 128 == 0
    near = [range(len(a)) for a, _, _ in tables]
    rest = [range(len(a), len(a) + len(b)) for a, b, _ in tables]
    cross = [r.stop for r in rest]
    extra = [range(c + 2, c + 2 + len(r)) for c, r in zip(cross, rest)]

    def inner(zz):
        return (zz != 0) & (zz != last)

    def rest_by_x(zz, here):
        return inner(zz) | (zz == here) | (zz + here == last)

    def goes(p, zz, k, right, here):
        if k < cross[p] + 2:
            return here < last if right else here > 0
        return (zz == 0) & (here + 1 < last) if right else (zz == last) & (here > 1)

    def settled(ref, sem):
        pltpu.make_async_copy(ref, ref, sem).wait()

    def settled_rows(count, sem):
        if count:
            tiles = count * width // 1024
            across = next(c for c in range(width // 128, 0, -1) if tiles % c == 0)
            settled(up_ref.at[pl.ds(0, tiles // across * 8), pl.ds(0, across * 128)], sem)

    def size_of(p, items):
        return sum(size * columns for _, size, _, columns in (tables[p][2][k] for k in items)) // width

    def at(p, col, zz, k):
        start, size, column, columns = tables[p][2][k]
        base = pl.multiple_of((col * n_fs + zz) * rows, rows)
        return masters[p].at[pl.ds(pl.multiple_of(base + start, 8), size), pl.ds(column, columns)]

    def kind(p, k):
        return p if tables[p][2][k][3] == width else 2

    def z_sem(p, zz, k, right):
        item = (len(tables[0][2]) if p else 0) + min(k, cross[p] + 2)
        return z_recv.at[zz if right else zz - 1, item]

    def z_copy(p, zz, k, right):
        ref = at(p, 1 - g if k > cross[p] else g, zz, k)
        send = right_send if right else left_send
        return pltpu.make_async_remote_copy(
            src_ref=ref, dst_ref=ref, send_sem=send.at[kind(p, k)], recv_sem=z_sem(p, zz, k, right),
            device_id=(g, jnp.where(has_right, z + 1, z - 1) if right else jnp.where(has_left, z - 1, z + 1), t),
            device_id_type=MESH,
        )

    def x_sem(p, zz, k):
        if k == cross[p]:
            return x_recv.at[p]
        if p == 0:
            return x_recv.at[2]
        return x_recv.at[3 + zz + (0 if k in near[1] else n_fs)]

    def x_copy(p, zz, k, col):
        ref = at(p, col, zz, k)
        return pltpu.make_async_remote_copy(
            src_ref=ref, dst_ref=ref, send_sem=x_send.at[kind(p, k)], recv_sem=x_sem(p, zz, k),
            device_id=(1 - g, z, t), device_id_type=MESH,
        )

    def send_both(p, k):
        pl.when(goes(p, z, k, True, z))(lambda: z_copy(p, z, k, True).start())
        pl.when(goes(p, z, k, False, z))(lambda: z_copy(p, z, k, False).start())

    def own_z(p):
        for k in range(cross[p] + 1):
            send_both(p, k)

    def own_x(p):
        for k in (cross[p], *rest[p], *near[p]):
            x_copy(p, z, k, g).start()

    def other_xz(p):
        x_copy(p, z, cross[p], 1 - g).wait_recv()
        send_both(p, cross[p] + 1)

    def near_in(zz):
        settled_rows(size_of(1, near[1]), x_recv.at[3 + zz])

    def rest_in(zz):
        settled_rows(size_of(1, rest[1]), x_recv.at[3 + n_fs + zz])

    def other_rest(p):
        @pl.when(at_end)
        def _():
            rest_in(z)
            for wide in extra[p]:
                send_both(p, wide)

    def slot(p, s, items):
        for k in items:
            wide = k in extra[p]
            if wide and (s == last or k > extra[p][0]):
                continue

            def come(right):
                zz = z - s if right else z + s
                if wide:
                    settled_rows(size_of(p, extra[p]), z_sem(p, zz, k, right))
                else:
                    z_copy(p, zz, k, right).wait_recv()
                if s < last:
                    @pl.when(goes(p, zz, k, right, z))
                    def _():
                        for item in extra[p] if wide else (k,):
                            z_copy(p, zz, item, right).start()

                if k in near[p]:
                    x_copy(p, zz, k, g).start()
                elif k in rest[p]:
                    pl.when(rest_by_x(zz, z))(lambda: x_copy(p, zz, k, g).start())

            from_left, from_right = z - s >= 0, z + s <= last
            if wide:
                from_left, from_right = (z - s == 0) & has_right, (z + s == last) & has_left
            pl.when(from_left)(lambda: come(True))
            pl.when(from_right)(lambda: come(False))

    def whole_slot(p, s):
        slot(p, s, range(len(tables[p][2])))

    def token_copy(j):
        mine = normed.at[pl.ds(pl.multiple_of(t * local, local), local), :]
        return pltpu.make_async_remote_copy(
            src_ref=mine, dst_ref=mine, send_sem=tok_sem.at[0], recv_sem=tok_sem.at[1],
            device_id=(g, z, lax.rem(t + j, n_tp)), device_id_type=MESH,
        )

    far = jnp.where(z + z >= last, 0, last)
    shares = [(0, tail), (tail, rows - tail)]
    whole_block = (0, rows)

    def part_copy(block, share, j, final):
        to = lax.rem(t + j, n_tp)
        start, size = share
        base = pl.multiple_of(block * rows, rows)
        row = pl.ds(pl.multiple_of(base + start, 16), size)
        return pltpu.make_async_remote_copy(
            src_ref=part.at[row, pl.ds(pl.multiple_of(to * local, local), local)],
            dst_ref=arrived.at[j - 1, row, :],
            send_sem=part_send.at[0], recv_sem=part_recv.at[1 if final else 0],
            device_id=(g, z, to), device_id_type=MESH,
        )

    def product(block, share, values):
        start, size = share
        base = pl.multiple_of(block * rows, rows)
        row = pl.ds(pl.multiple_of(base + start, 16), size)
        return row, lax.dot_general(
            down_ref[row, :], values[...], (((1,), (1,)), ((), ())),
            preferred_element_type=jnp.float32,
        ).astype(part.dtype)

    def multiply(block, share, final=False):
        row, value = product(block, share, hidden)
        part[row, :] = value
        for j in range(1, n_tp):
            part_copy(block, share, j, final).start()

    def second(s):
        def one(i, carry):
            other, side = i // 2, lax.rem(i, 2)
            dist = s - other
            zz = z + (2 * side - 1) * dist
            ok = (dist >= 0) & (zz >= 0) & (zz <= last) & ((dist > 0) | (side == 0)) & (zz != far)

            @pl.when(ok)
            def _():
                @pl.when(other == 1)
                def _():
                    near_in(zz)
                    pl.when(inner(zz))(lambda: rest_in(zz))

                multiply(jnp.where(other == 1, 1 - g, g) * n_fs + zz, whole_block)

            return carry

        lax.fori_loop(0, 4, one, 0)

    def far_share(col, i, final=False):
        if shares[i][1] > 0:
            multiply(col * n_fs + far, shares[i], final)

    def far_tails():
        far_share(g, 1)
        far_share(1 - g, 1)

    tail_here = jnp.logical_not(at_end) if helped else z >= 0
    helping = (z == 1) | (z == last - 1)
    helper = jnp.where(z == 0, 1, last - 1)
    ward = jnp.where(z == 1, 0, last)

    def hidden_copy():
        return pltpu.make_async_remote_copy(
            src_ref=hidden, dst_ref=far_hidden, send_sem=hid_sem.at[0], recv_sem=hid_sem.at[1],
            device_id=(g, helper, t), device_id_type=MESH,
        )

    def far_copy(col, j):
        to = lax.rem(t + j, n_tp)
        row = pl.ds(col * 128, 128)
        return pltpu.make_async_remote_copy(
            src_ref=far_part.at[row, pl.ds(pl.multiple_of(to * local, local), local)],
            dst_ref=far_arrived.at[j - 1, row, :],
            send_sem=far_sem.at[0], recv_sem=far_sem.at[1],
            device_id=(g, z, to), device_id_type=MESH,
        )

    def give_copy(col):
        column = pl.ds(pl.multiple_of((col * n_fs + far) * rows + tail, 128), 128)
        return pltpu.make_async_remote_copy(
            src_ref=far_out.at[col], dst_ref=out_ref.at[:, column],
            send_sem=give_sem.at[0], recv_sem=give_sem.at[1],
            device_id=(g, ward, t), device_id_type=MESH,
        )

    def help_multiply():
        hidden_copy().wait_recv()
        for col in range(2):
            _, value = product(col * n_fs + far, shares[1], far_hidden)
            far_part[pl.ds(col * 128, 128), :] = value
            for j in range(1, n_tp):
                far_copy(col, j).start()

    def help_total():
        settled(far_arrived, far_sem.at[1])
        for col in range(2):
            row = pl.ds(col * 128, 128)
            acc = far_part[row, pl.ds(pl.multiple_of(t * local, local), local)].astype(jnp.float32)
            for j in range(1, n_tp):
                acc = acc + far_arrived[j - 1, row, :].astype(jnp.float32)
            far_out[col] = acc.T.astype(far_out.dtype)
            give_copy(col).start()

    def parts_settled(final_rows, sem):
        every = depth - final_rows
        if not helped:
            settled(arrived.at[:, pl.ds(0, every), :], sem)
            return
        pl.when(at_end)(lambda: settled(arrived.at[:, pl.ds(0, every - 256), :], sem))
        pl.when(tail_here)(lambda: settled(arrived.at[:, pl.ds(0, every), :], sem))

    barrier = pltpu.get_barrier_semaphore()

    def greet(device):
        pl.semaphore_signal(barrier, inc=1, device_id=device, device_id_type=MESH)

    greet((1 - g, z, t))
    pl.when(has_right)(lambda: greet((g, z + 1, t)))
    pl.when(has_left)(lambda: greet((g, z - 1, t)))
    for j in range(1, n_tp):
        greet((g, z, lax.rem(t + j, n_tp)))

    order = [cross[0], *near[0]]

    def up_load(k):
        start, size = tables[0][2][k][:2]
        row = pl.ds(start, size)
        return pltpu.make_async_copy(up_hbm.at[row, :], stage.at[0, row, :], up_sem.at[k])

    loads = [
        pltpu.make_async_copy(gain_hbm, gain_ref, load_sem.at[0]),
        pltpu.make_async_copy(tok_hbm, tok_ref, load_sem.at[1]),
        pltpu.make_async_copy(down_hbm, stage.at[1], load_sem.at[2]),
    ]
    loads[0].start()
    for k in order:
        up_load(k).start()
    loads[1].start()
    loads[2].start()

    def round_up(k):
        start, size = tables[0][2][k][:2]
        row = pl.ds(pl.multiple_of((g * n_fs + z) * rows + start, 8), size)
        up_load(k).wait()
        up_ref[row, :] = (stage[0, start : start + size] * gain[start : start + size]).astype(up_ref.dtype)

    def send_own(k):
        x_copy(0, z, k, g).start()
        if k != cross[0]:
            send_both(0, k)

    own = pl.ds(pl.multiple_of((g * n_fs + z) * rows, rows), rows)
    square = (rows, rows)
    on_diagonal = lax.broadcasted_iota(jnp.int32, square, 0) == lax.broadcasted_iota(jnp.int32, square, 1)
    loads[0].wait()
    gain = jnp.sum(jnp.where(on_diagonal, gain_ref[...], 0.0), axis=1, keepdims=True)
    round_up(order[0])
    round_up(order[1])
    pl.semaphore_wait(barrier, n_tp + has_right.astype(jnp.int32) + has_left.astype(jnp.int32))
    for i, k in enumerate(order):
        send_own(k)
        if i + 2 < len(order):
            round_up(order[i + 2])
    send_both(0, cross[0])

    loads[1].wait()
    floats = tok_ref[...].astype(jnp.float32)
    mean_square = jnp.mean(floats * floats, axis=1, keepdims=True)
    normed[pl.ds(pl.multiple_of(t * local, local), local), :] = (
        floats * lax.rsqrt(mean_square + 1e-06)
    ).astype(normed.dtype)
    for j in range(1, n_tp):
        token_copy(j).start()
    other_xz(0)
    loads[2].wait()
    down_ref[own, :] = stage[1].astype(down_ref.dtype)

    for s in range(1, last):
        whole_slot(0, s)
    own_z(1)
    if last > 0:
        slot(0, last, near[0])
    own_x(1)
    if last > 0:
        slot(0, last, range(cross[0], cross[0] + 2))

    settled_rows(n_fs * size_of(0, near[0]), x_recv.at[2])
    others = normed.at[pl.ds(0, (n_tp - 1) * local), :]
    settled(others, tok_sem.at[1])

    tile = 256

    def first(i, carry):
        columns = pl.ds(pl.multiple_of(i * tile, tile), tile)
        pre = jnp.dot(normed[...], up_ref[:, columns], preferred_element_type=jnp.float32)
        hidden[:, columns] = jnp.square(jnp.maximum(pre, 0.0)).astype(hidden.dtype)
        return carry

    lax.fori_loop(0, width // tile, first, 0)

    other_xz(1)
    other_rest(1)
    if helped:
        @pl.when(at_end)
        def _():
            hidden_copy().start()

    second(0)
    for s in range(1, last):
        whole_slot(1, s)
        second(s)
    slot(1, last, near[1])
    second(last)
    far_share(g, 0)
    slot(1, last, rest[1])
    if helped:
        pl.when(tail_here)(far_tails)
        pl.when(helping)(help_multiply)
    near_in(far)
    far_share(1 - g, 0, True)
    if helped:
        pl.when(helping)(help_total)

    def last_in():
        slot(1, last, range(cross[1], cross[1] + 2))

        pl.when(at_end)(lambda: rest_in(far))

    if not helped:
        last_in()
        far_tails()

    final = (1 - g) * n_fs + far
    final_tile = final * (rows // 128)
    last_tile = final_tile + tail // 128

    parts_settled(tail, part_recv.at[0])

    def total(i, carry):
        row = pl.ds(pl.multiple_of(i * 128, 128), 128)
        acc = part[row, pl.ds(pl.multiple_of(t * local, local), local)].astype(jnp.float32)
        for j in range(1, n_tp):
            acc = acc + arrived[j - 1, row, :].astype(jnp.float32)
        out_ref[:, row] = acc.T.astype(out_ref.dtype)
        return carry

    def total_if(i, carry):
        is_tail = (lax.rem(i * 128, rows) == tail) & (lax.rem(i * 128 // rows, n_fs) == far)

        @pl.when(tail_here | jnp.logical_not(is_tail))
        def _():
            total(i, 0)

        return carry

    lax.fori_loop(0, final_tile, total_if, 0)
    lax.fori_loop(last_tile, depth // 128, total_if, 0)

    if tail > 0:
        settled(arrived.at[:, pl.ds(0, tail), :], part_recv.at[1])
    lax.fori_loop(final_tile, last_tile, total, 0)
    parts_settled(0, part_send.at[0])
    settled(others, tok_sem.at[0])
    if helped:
        pl.when(at_end)(lambda: hidden_copy().wait_send())
        pl.when(helping)(lambda: settled(far_arrived, far_sem.at[0]))

    def sent_blocks(here):
        sent = [[0, 0, 0] for _ in range(3)]
        for p in range(2):
            for zz in range(n_fs):
                for k in range(len(tables[p][2])):
                    size, to = size_of(p, [k]), kind(p, k)
                    by_x = k in near[p] or (k in rest[p] and rest_by_x(zz, here)) or (k <= cross[p] and zz == here)
                    sent[0][to] += size * (zz <= here and goes(p, zz, k, True, here))
                    sent[1][to] += size * (zz >= here and goes(p, zz, k, False, here))
                    sent[2][to] += size * by_x
        for counts, sem in zip(sent, (right_send, left_send, x_send)):
            for to, count in enumerate(counts):
                settled_rows(count, sem.at[to])

    for here in range(n_fs):
        pl.when(z == here)(functools.partial(sent_blocks, here))
    if helped:
        last_in()

        pl.when(at_end)(lambda: settled(far_out, give_sem.at[1]))
        pl.when(helping)(lambda: settled(far_out, give_sem.at[0]))


def write_out(*refs):
    held, outs, sem = refs[:3], refs[3:6], refs[6]
    for i, (src, dst) in enumerate(zip(held, outs)):
        rows = src.shape[0] // WRITES
        for k in range(WRITES):
            part = pl.ds(k * rows, rows)
            pltpu.make_async_copy(src.at[part, :], dst.at[part, :], sem.at[i]).start()
    for i, (src, dst) in enumerate(zip(held, outs)):
        pltpu.make_async_copy(src, dst, sem.at[i]).wait()


def solution(mesh):
    n_gr, n_fs, n_tp = (mesh.shape[a] for a in ("gr", "fs", "tp"))

    def on_device(prompt_tokens, norm_gain, up_master, down_master):
        local, depth = prompt_tokens.shape
        rows, width = up_master.shape
        ups, downs = (len(table) for _, _, table in split_rows(rows, width)[1])
        dma = pltpu.SemaphoreType.DMA
        bf16 = jnp.bfloat16
        anywhere = pl.BlockSpec(memory_space=pl.ANY)
        vmem = pl.BlockSpec(memory_space=pltpu.VMEM)
        held = pl.pallas_call(
            functools.partial(kernel, (n_gr, n_fs, n_tp)),
            out_shape=(
                pltpu.VMEM((depth, width), bf16),
                pltpu.VMEM((depth, width), bf16),
                pltpu.VMEM((local, depth), bf16),
            ),
            in_specs=[anywhere] * 4,
            out_specs=(vmem, vmem, vmem),
            scratch_shapes=[
                pltpu.VMEM((local, depth), bf16),
                pltpu.VMEM((1, rows), jnp.float32),
                pltpu.VMEM((2, rows, width), jnp.float32),
                pltpu.VMEM((local * n_tp, depth), bf16),
                pltpu.VMEM((local * n_tp, width), bf16),
                pltpu.VMEM((depth, local * n_tp), bf16),
                pltpu.VMEM((n_tp - 1, depth, local), bf16),
                pltpu.VMEM((local * n_tp, width), bf16),
                pltpu.VMEM((256, local * n_tp), bf16),
                pltpu.VMEM((n_tp - 1, 256, local), bf16),
                pltpu.VMEM((2, local, 128), bf16),
                dma((3,)), dma((ups,)), dma((2,)),
                dma((max(1, n_fs - 1), ups + downs)), dma((3,)), dma((3,)), dma((3 + 2 * n_fs,)), dma((3,)),
                dma((1,)), dma((2,)), dma((2,)), dma((2,)), dma((2,)),
            ],
            compiler_params=pltpu.CompilerParams(
                collective_id=0, has_side_effects=True, vmem_limit_bytes=44 * 2**20
            ),
        )(norm_gain[None, :], prompt_tokens, up_master, down_master)
        return pl.pallas_call(
            write_out,
            out_shape=(
                jax.ShapeDtypeStruct((depth, width), bf16),
                jax.ShapeDtypeStruct((depth, width), bf16),
                jax.ShapeDtypeStruct((local, depth), bf16),
            ),
            in_specs=[vmem, vmem, vmem],
            out_specs=(anywhere, anywhere, anywhere),
            scratch_shapes=[dma((3,))],
            compiler_params=pltpu.CompilerParams(vmem_limit_bytes=2**20),
        )(*held)

    placed = (
        P(("gr", "fs", "tp"), None),
        P(("gr", "fs")),
        P(("gr", "fs"), "tp"),
        P(("gr", "fs"), "tp"),
    )
    return jax.shard_map(
        on_device,
        mesh=mesh,
        in_specs=placed,
        out_specs=(P(None, "tp"), P(None, "tp"), P(("gr", "fs", "tp"), None)),
        check_vma=False,
    )
```

```python
import functools

import jax
import jax.numpy as jnp
from jax import lax
from jax.experimental import pallas as pl
from jax.experimental.pallas import tpu as pltpu
from jax.sharding import PartitionSpec as P

MESH = pl.DeviceIdType.MESH
PIECES = (3, 2, 1)
WRITES = 4
DELAY = 19000


def pieces_of(start, stop, count):
    units = (stop - start) // 8
    cuts = [start + 8 * (units * i // count) for i in range(count)] + [stop]
    return [(a, b - a) for a, b in zip(cuts, cuts[1:]) if b > a]


def split_rows(rows, width):
    def wide(pieces):
        return [(start, size, 0, width) for start, size in pieces]

    tail = max(0, rows - 128)
    edge = rows - max(8, rows * 5 // 256 * 8)
    near, cross = wide(pieces_of(0, edge, PIECES[0])), wide([(edge, rows - edge)])
    tables = [(near, [], near + cross + cross)]
    edge = rows - max(8, rows * 6 // 256 * 8)
    column = width * 7 // 8 // 128 * 128
    cut = min(tail, edge)
    near, rest = wide(pieces_of(0, cut, PIECES[1])), wide(pieces_of(cut, edge, PIECES[2]))
    rest.append((edge, rows - edge, column, width - column))
    cross = [(edge, rows - edge, 0, column)]
    tables.append((near, rest, near + rest + cross + cross + rest))
    return tail, tables


def kernel(phase, sizes, *refs):
    if phase == 0:
        (gain_hbm, tok_hbm, up_hbm, up_ref, normed, tok_ref, gain_ref, stage, load_sem, up_sem, tok_sem,
         z_recv, right_send, left_send, x_recv, x_send) = refs
        master = up_ref
    else:
        (up_ref, normed, stage, _, down_ref, out_ref, hidden, part, arrived,
         far_hidden, far_part, far_arrived, far_out,
         z_recv, right_send, left_send, x_recv, x_send, part_send, part_recv,
         hid_sem, far_sem, give_sem, late_sem) = refs
        master = down_ref
    n_gr, n_fs, n_tp = sizes
    g, z, t = lax.axis_index("gr"), lax.axis_index("fs"), lax.axis_index("tp")
    rows, width = stage.shape
    local = normed.shape[0] // n_tp
    depth = up_ref.shape[0]
    odd = lax.rem(t, 2) == 1
    last = n_fs - 1
    has_right, has_left = z < last, z > 0
    at_end = (z == 0) | (z == last)

    tail, tables = split_rows(rows, width)
    helped = n_fs >= 4 and rows % 128 == 0
    near = [range(len(a)) for a, _, _ in tables]
    rest = [range(len(a), len(a) + len(b)) for a, b, _ in tables]
    cross = [r.stop for r in rest]
    extra = [range(c + 2, c + 2 + len(r)) for c, r in zip(cross, rest)]

    def inner(zz):
        return (zz != 0) & (zz != last)

    def rest_by_x(zz, here):
        return inner(zz) | (zz == here) | (zz + here == last)

    def goes(p, zz, k, right, here):
        if k < cross[p] + 2:
            return here < last if right else here > 0
        return (zz == 0) & (here + 1 < last) if right else (zz == last) & (here > 1)

    def settled(ref, sem):
        pltpu.make_async_copy(ref, ref, sem).wait()

    def settled_rows(count, sem):
        if count:
            tiles = count * width // 1024
            across = next(c for c in range(width // 128, 0, -1) if tiles % c == 0)
            settled(master.at[pl.ds(0, tiles // across * 8), pl.ds(0, across * 128)], sem)

    def size_of(p, items):
        return sum(size * columns for _, size, _, columns in (tables[p][2][k] for k in items)) // width

    def at(p, col, zz, k):
        start, size, column, columns = tables[p][2][k]
        base = pl.multiple_of((col * n_fs + zz) * rows, rows)
        return master.at[pl.ds(pl.multiple_of(base + start, 8), size), pl.ds(column, columns)]

    def kind(p, k):
        return 0 if tables[p][2][k][3] == width else 1

    def z_sem(p, zz, k, right):
        return z_recv.at[zz if right else zz - 1, min(k, cross[p] + 2)]

    def z_copy(p, zz, k, right):
        ref = at(p, 1 - g if k > cross[p] else g, zz, k)
        send = right_send if right else left_send
        return pltpu.make_async_remote_copy(
            src_ref=ref, dst_ref=ref, send_sem=send.at[kind(p, k)], recv_sem=z_sem(p, zz, k, right),
            device_id=(g, jnp.where(has_right, z + 1, z - 1) if right else jnp.where(has_left, z - 1, z + 1), t),
            device_id_type=MESH,
        )

    def x_sem(p, zz, k):
        if k == cross[p]:
            return x_recv.at[0]
        if p == 0:
            return x_recv.at[1]
        return x_recv.at[1 + zz + (0 if k in near[1] else n_fs)]

    def x_copy(p, zz, k, col):
        ref = at(p, col, zz, k)
        return pltpu.make_async_remote_copy(
            src_ref=ref, dst_ref=ref, send_sem=x_send.at[kind(p, k)], recv_sem=x_sem(p, zz, k),
            device_id=(1 - g, z, t), device_id_type=MESH,
        )

    def send_both(p, k):
        pl.when(goes(p, z, k, True, z))(lambda: z_copy(p, z, k, True).start())
        pl.when(goes(p, z, k, False, z))(lambda: z_copy(p, z, k, False).start())

    def own_z(p):
        for k in range(cross[p] + 1):
            send_both(p, k)

    def own_x(p):
        for k in (cross[p], *rest[p], *near[p]):
            x_copy(p, z, k, g).start()

    def other_xz(p):
        x_copy(p, z, cross[p], 1 - g).wait_recv()
        send_both(p, cross[p] + 1)

    def near_in(zz):
        settled_rows(size_of(1, near[1]), x_recv.at[1 + zz])

    def rest_in(zz):
        settled_rows(size_of(1, rest[1]), x_recv.at[1 + n_fs + zz])

    def other_rest(p):
        @pl.when(at_end)
        def _():
            rest_in(z)
            for wide in extra[p]:
                send_both(p, wide)

    def slot(p, s, items):
        for k in items:
            wide = k in extra[p]
            if wide and (s == last or k > extra[p][0]):
                continue

            def come(right):
                zz = z - s if right else z + s
                if wide:
                    settled_rows(size_of(p, extra[p]), z_sem(p, zz, k, right))
                else:
                    z_copy(p, zz, k, right).wait_recv()
                if s < last:
                    @pl.when(goes(p, zz, k, right, z))
                    def _():
                        for item in extra[p] if wide else (k,):
                            z_copy(p, zz, item, right).start()

                if k in near[p]:
                    x_copy(p, zz, k, g).start()
                elif k in rest[p]:
                    pl.when(rest_by_x(zz, z))(lambda: x_copy(p, zz, k, g).start())

            from_left, from_right = z - s >= 0, z + s <= last
            if wide:
                from_left, from_right = (z - s == 0) & has_right, (z + s == last) & has_left
            pl.when(from_left)(lambda: come(True))
            pl.when(from_right)(lambda: come(False))

    def whole_slot(p, s):
        slot(p, s, range(len(tables[p][2])))

    def token_copy(j):
        mine = normed.at[pl.ds(pl.multiple_of(t * local, local), local), :]
        return pltpu.make_async_remote_copy(
            src_ref=mine, dst_ref=mine, send_sem=tok_sem.at[0], recv_sem=tok_sem.at[1],
            device_id=(g, z, lax.rem(t + j, n_tp)), device_id_type=MESH,
        )

    far = jnp.where(z + z >= last, 0, last)
    shares = [(0, tail), (tail, rows - tail)]
    whole_block = (0, rows)

    def part_copy(block, share, j, final):
        to = lax.rem(t + j, n_tp)
        start, size = share
        base = pl.multiple_of(block * rows, rows)
        row = pl.ds(pl.multiple_of(base + start, 16), size)
        return pltpu.make_async_remote_copy(
            src_ref=part.at[row, pl.ds(pl.multiple_of(to * local, local), local)],
            dst_ref=arrived.at[j - 1, row, :],
            send_sem=part_send.at[0], recv_sem=part_recv.at[1 if final else 0],
            device_id=(g, z, to), device_id_type=MESH,
        )

    def product(block, share, values):
        start, size = share
        base = pl.multiple_of(block * rows, rows)
        row = pl.ds(pl.multiple_of(base + start, 16), size)
        return row, lax.dot_general(
            down_ref[row, :], values[...], (((1,), (1,)), ((), ())),
            preferred_element_type=jnp.float32,
        ).astype(part.dtype)

    def multiply(block, share, final=False):
        row, value = product(block, share, hidden)
        part[row, :] = value
        for j in range(1, n_tp):
            part_copy(block, share, j, final).start()

    def second(s):
        def one(i, carry):
            other, side = i // 2, lax.rem(i, 2)
            dist = s - other
            zz = z + (2 * side - 1) * dist
            ok = (dist >= 0) & (zz >= 0) & (zz <= last) & ((dist > 0) | (side == 0)) & (zz != far)

            @pl.when(ok)
            def _():
                @pl.when(other == 1)
                def _():
                    near_in(zz)
                    pl.when(inner(zz))(lambda: rest_in(zz))

                multiply(jnp.where(other == 1, 1 - g, g) * n_fs + zz, whole_block)

            return carry

        lax.fori_loop(0, 4, one, 0)

    def far_share(col, i, final=False):
        if shares[i][1] > 0:
            multiply(col * n_fs + far, shares[i], final)

    def far_tails():
        far_share(g, 1)
        far_share(1 - g, 1)

    tail_here = jnp.logical_not(at_end) if helped else z >= 0
    helping = (z == 1) | (z == last - 1)
    helper = jnp.where(z == 0, 1, last - 1)
    ward = jnp.where(z == 1, 0, last)

    def hidden_copy():
        return pltpu.make_async_remote_copy(
            src_ref=hidden, dst_ref=far_hidden, send_sem=hid_sem.at[0], recv_sem=hid_sem.at[1],
            device_id=(g, helper, t), device_id_type=MESH,
        )

    def far_copy(col, j):
        to = lax.rem(t + j, n_tp)
        row = pl.ds(col * 128, 128)
        return pltpu.make_async_remote_copy(
            src_ref=far_part.at[row, pl.ds(pl.multiple_of(to * local, local), local)],
            dst_ref=far_arrived.at[j - 1, row, :],
            send_sem=far_sem.at[0], recv_sem=far_sem.at[1],
            device_id=(g, z, to), device_id_type=MESH,
        )

    def give_copy(col):
        column = pl.ds(pl.multiple_of((col * n_fs + far) * rows + tail, 128), 128)
        return pltpu.make_async_remote_copy(
            src_ref=far_out.at[col], dst_ref=out_ref.at[:, column],
            send_sem=give_sem.at[0], recv_sem=give_sem.at[1],
            device_id=(g, ward, t), device_id_type=MESH,
        )

    def help_multiply():
        hidden_copy().wait_recv()
        for col in range(2):
            _, value = product(col * n_fs + far, shares[1], far_hidden)
            far_part[pl.ds(col * 128, 128), :] = value
            for j in range(1, n_tp):
                far_copy(col, j).start()

    def help_total():
        settled(far_arrived, far_sem.at[1])
        for col in range(2):
            row = pl.ds(col * 128, 128)
            acc = far_part[row, pl.ds(pl.multiple_of(t * local, local), local)].astype(jnp.float32)
            for j in range(1, n_tp):
                acc = acc + far_arrived[j - 1, row, :].astype(jnp.float32)
            far_out[col] = acc.T.astype(far_out.dtype)
            give_copy(col).start()

    def parts_settled(final_rows, sem):
        every = depth - final_rows
        if not helped:
            settled(arrived.at[:, pl.ds(0, every), :], sem)
            return
        pl.when(at_end)(lambda: settled(arrived.at[:, pl.ds(0, every - 256), :], sem))
        pl.when(tail_here)(lambda: settled(arrived.at[:, pl.ds(0, every), :], sem))

    def sent_blocks(p, here):
        sent = [[0, 0] for _ in range(3)]
        for zz in range(n_fs):
            for k in range(len(tables[p][2])):
                size, to = size_of(p, [k]), kind(p, k)
                by_x = k in near[p] or (k in rest[p] and rest_by_x(zz, here)) or (k <= cross[p] and zz == here)
                sent[0][to] += size * (zz <= here and goes(p, zz, k, True, here))
                sent[1][to] += size * (zz >= here and goes(p, zz, k, False, here))
                sent[2][to] += size * by_x
        for counts, sem in zip(sent, (right_send, left_send, x_send)):
            for to, count in enumerate(counts):
                settled_rows(count, sem.at[to])

    def all_sent(p):
        for here in range(n_fs):
            pl.when(z == here)(functools.partial(sent_blocks, p, here))

    barrier = pltpu.get_barrier_semaphore()

    def greet(device):
        pl.semaphore_signal(barrier, inc=1, device_id=device, device_id_type=MESH)

    greet((1 - g, z, t))
    pl.when(has_right)(lambda: greet((g, z + 1, t)))
    pl.when(has_left)(lambda: greet((g, z - 1, t)))
    for j in range(1, n_tp):
        if phase == 0 or j % 2 == 0:
            greet((g, z, lax.rem(t + j, n_tp)))
        else:
            pl.when(jnp.logical_not(odd))(functools.partial(greet, (g, z, lax.rem(t + j, n_tp))))

    def gather_up():
        order = [cross[0], *near[0]]

        def up_load(k):
            start, size = tables[0][2][k][:2]
            row = pl.ds(start, size)
            return pltpu.make_async_copy(up_hbm.at[row, :], stage.at[row, :], up_sem.at[k])

        loads = [
            pltpu.make_async_copy(gain_hbm, gain_ref, load_sem.at[0]),
            pltpu.make_async_copy(tok_hbm, tok_ref, load_sem.at[1]),
        ]
        loads[0].start()
        for k in order:
            up_load(k).start()
        loads[1].start()

        def round_up(k):
            start, size = tables[0][2][k][:2]
            row = pl.ds(pl.multiple_of((g * n_fs + z) * rows + start, 8), size)
            up_load(k).wait()
            up_ref[row, :] = (stage[start : start + size] * gain[start : start + size]).astype(up_ref.dtype)

        def send_own(k):
            x_copy(0, z, k, g).start()
            if k != cross[0]:
                send_both(0, k)

        square = (rows, rows)
        on_diagonal = lax.broadcasted_iota(jnp.int32, square, 0) == lax.broadcasted_iota(jnp.int32, square, 1)
        loads[0].wait()
        gain = jnp.sum(jnp.where(on_diagonal, gain_ref[...], 0.0), axis=1, keepdims=True)
        round_up(order[0])
        round_up(order[1])
        pl.semaphore_wait(barrier, n_tp + has_right.astype(jnp.int32) + has_left.astype(jnp.int32))
        pl.when(odd)(lambda: pl.delay(DELAY))
        for i, k in enumerate(order):
            send_own(k)
            if i + 2 < len(order):
                round_up(order[i + 2])
        send_both(0, cross[0])

        loads[1].wait()
        floats = tok_ref[...].astype(jnp.float32)
        mean_square = jnp.mean(floats * floats, axis=1, keepdims=True)
        normed[pl.ds(pl.multiple_of(t * local, local), local), :] = (
            floats * lax.rsqrt(mean_square + 1e-06)
        ).astype(normed.dtype)
        for j in range(1, n_tp):
            token_copy(j).start()
        other_xz(0)

        for s in range(1, last + 1):
            whole_slot(0, s)
        settled_rows(n_fs * size_of(0, near[0]), x_recv.at[1])
        others = normed.at[pl.ds(0, (n_tp - 1) * local), :]
        settled(others, tok_sem.at[1])
        settled(others, tok_sem.at[0])
        all_sent(0)

    def gather_down():
        def late(device):
            pl.semaphore_signal(late_sem, inc=1, device_id=device, device_id_type=MESH)

        own = pl.ds(pl.multiple_of((g * n_fs + z) * rows, rows), rows)
        down_ref[own, :] = stage[...].astype(down_ref.dtype)
        sides = has_right.astype(jnp.int32) + has_left.astype(jnp.int32)
        pl.semaphore_wait(barrier, n_tp // 2 + sides + odd.astype(jnp.int32) * (n_tp // 2))
        own_z(1)
        own_x(1)

        @pl.when(odd)
        def _():
            for j in range(1, n_tp, 2):
                late((g, z, lax.rem(t + j, n_tp)))

        tile = 256

        def first(i, carry):
            columns = pl.ds(pl.multiple_of(i * tile, tile), tile)
            pre = jnp.dot(normed[...], up_ref[:, columns], preferred_element_type=jnp.float32)
            hidden[:, columns] = jnp.square(jnp.maximum(pre, 0.0)).astype(hidden.dtype)
            return carry

        lax.fori_loop(0, width // tile, first, 0)
        wait_late = lambda: pl.semaphore_wait(late_sem, n_tp // 2)
        other_xz(1)
        other_rest(1)
        if helped:
            @pl.when(at_end)
            def _():
                hidden_copy().start()

        for s in range(1, last):
            whole_slot(1, s)
            if s == 1:
                pl.when(jnp.logical_not(odd))(wait_late)
                second(0)
            second(s)
        slot(1, last, near[1])
        second(last)
        far_share(g, 0)
        slot(1, last, rest[1])
        if helped:
            pl.when(tail_here)(far_tails)
            pl.when(helping)(help_multiply)
        near_in(far)
        far_share(1 - g, 0, True)
        if helped:
            pl.when(helping)(help_total)

        def last_in():
            slot(1, last, range(cross[1], cross[1] + 2))

            pl.when(at_end)(lambda: rest_in(far))

        if not helped:
            last_in()
            far_tails()

        final = (1 - g) * n_fs + far
        final_tile = final * (rows // 128)
        last_tile = final_tile + tail // 128

        parts_settled(tail, part_recv.at[0])

        def total(i, carry):
            row = pl.ds(pl.multiple_of(i * 128, 128), 128)
            acc = part[row, pl.ds(pl.multiple_of(t * local, local), local)].astype(jnp.float32)
            for j in range(1, n_tp):
                acc = acc + arrived[j - 1, row, :].astype(jnp.float32)
            out_ref[:, row] = acc.T.astype(out_ref.dtype)
            return carry

        def total_if(i, carry):
            is_tail = (lax.rem(i * 128, rows) == tail) & (lax.rem(i * 128 // rows, n_fs) == far)

            @pl.when(tail_here | jnp.logical_not(is_tail))
            def _():
                total(i, 0)

            return carry

        lax.fori_loop(0, final_tile, total_if, 0)
        lax.fori_loop(last_tile, depth // 128, total_if, 0)

        if tail > 0:
            settled(arrived.at[:, pl.ds(0, tail), :], part_recv.at[1])
        lax.fori_loop(final_tile, last_tile, total, 0)
        parts_settled(0, part_send.at[0])
        if helped:
            pl.when(at_end)(lambda: hidden_copy().wait_send())
            pl.when(helping)(lambda: settled(far_arrived, far_sem.at[0]))

        all_sent(1)
        if helped:
            last_in()

            pl.when(at_end)(lambda: settled(far_out, give_sem.at[1]))
            pl.when(helping)(lambda: settled(far_out, give_sem.at[0]))

    gather_up() if phase == 0 else gather_down()


def write_out(count, *refs):
    held, outs, sem = refs[:count], refs[count : 2 * count], refs[-1]
    for i, (src, dst) in enumerate(zip(held, outs)):
        rows = src.shape[0] // WRITES
        for k in range(WRITES):
            part = pl.ds(k * rows, rows)
            pltpu.make_async_copy(src.at[part, :], dst.at[part, :], sem.at[i]).start()
    if len(refs) > 2 * count + 1:
        refs[2 * count][...] = jnp.zeros_like(refs[2 * count])
    for i, (src, dst) in enumerate(zip(held, outs)):
        pltpu.make_async_copy(src, dst, sem.at[i]).wait()


def solution(mesh):
    n_gr, n_fs, n_tp = (mesh.shape[a] for a in ("gr", "fs", "tp"))

    def on_device(prompt_tokens, norm_gain, up_master, down_master):
        local, depth = prompt_tokens.shape
        rows, width = up_master.shape
        ups, downs = (len(table) for _, _, table in split_rows(rows, width)[1])
        dma = pltpu.SemaphoreType.DMA
        bf16 = jnp.bfloat16
        anywhere = pl.BlockSpec(memory_space=pl.ANY)
        vmem = pl.BlockSpec(memory_space=pltpu.VMEM)
        main = pl.BlockSpec(memory_space=pltpu.HBM)
        sends = [dma((2,)), dma((2,))]

        weights, tokens, third = depth * width * 2, local * n_tp * depth * 2, local * n_tp * width * 2
        limits = (64 * 2**20 - weights - tokens - 2**18, 2 * third + rows * width * 4 + 3 * tokens + 8 * 2**20)

        def remote(phase):
            return pltpu.CompilerParams(collective_id=phase, has_side_effects=True, vmem_limit_bytes=limits[phase])

        kept = functools.partial(pltpu.with_memory_space_constraint, memory_space=pltpu.VMEM)
        small = pltpu.CompilerParams(vmem_limit_bytes=2**20)
        up, normed = pl.pallas_call(
            functools.partial(kernel, 0, (n_gr, n_fs, n_tp)),
            out_shape=(pltpu.VMEM((depth, width), bf16), pltpu.VMEM((local * n_tp, depth), bf16)),
            in_specs=[main] * 3,
            out_specs=(vmem, vmem),
            scratch_shapes=[
                pltpu.VMEM((local, depth), bf16),
                pltpu.VMEM((1, rows), jnp.float32),
                pltpu.VMEM((rows, width), jnp.float32),
                dma((2,)), dma((ups,)), dma((2,)),
                dma((max(1, n_fs - 1), ups)), *sends, dma((2,)), dma((2,)),
            ],
            compiler_params=remote(0),
        )(norm_gain[None, :], prompt_tokens, up_master)
        up_served, after = pl.pallas_call(
            functools.partial(write_out, 1),
            out_shape=(jax.ShapeDtypeStruct((depth, width), bf16), pltpu.VMEM((8, 128), jnp.float32)),
            in_specs=[vmem],
            out_specs=(anywhere, vmem),
            scratch_shapes=[dma((1,))],
            compiler_params=small,
        )(up)
        down, out = pl.pallas_call(
            functools.partial(kernel, 1, (n_gr, n_fs, n_tp)),
            out_shape=(pltpu.VMEM((depth, width), bf16), pltpu.VMEM((local, depth), bf16)),
            in_specs=[vmem] * 4,
            out_specs=(vmem, vmem),
            scratch_shapes=[
                pltpu.VMEM((local * n_tp, width), bf16),
                pltpu.VMEM((depth, local * n_tp), bf16),
                pltpu.VMEM((n_tp - 1, depth, local), bf16),
                pltpu.VMEM((local * n_tp, width), bf16),
                pltpu.VMEM((256, local * n_tp), bf16),
                pltpu.VMEM((n_tp - 1, 256, local), bf16),
                pltpu.VMEM((2, local, 128), bf16),
                dma((max(1, n_fs - 1), downs)), *sends, dma((1 + 2 * n_fs,)), dma((2,)),
                dma((1,)), dma((2,)), dma((2,)), dma((2,)), dma((2,)), pltpu.SemaphoreType.REGULAR,
            ],
            compiler_params=remote(1),
        )(kept(up), kept(normed), down_master, after)
        down_served, mlp_output = pl.pallas_call(
            functools.partial(write_out, 2),
            out_shape=(jax.ShapeDtypeStruct((depth, width), bf16), jax.ShapeDtypeStruct((local, depth), bf16)),
            in_specs=[vmem, vmem],
            out_specs=(anywhere, anywhere),
            scratch_shapes=[dma((2,))],
            compiler_params=small,
        )(down, out)
        return up_served, down_served, mlp_output

    placed = (
        P(("gr", "fs", "tp"), None),
        P(("gr", "fs")),
        P(("gr", "fs"), "tp"),
        P(("gr", "fs"), "tp"),
    )
    return jax.shard_map(
        on_device,
        mesh=mesh,
        in_specs=placed,
        out_specs=(P(None, "tp"), P(None, "tp"), P(("gr", "fs", "tp"), None)),
        check_vma=False,
    )
```
